256 devices in a mesh: sp: 64 (over z, x, core), tp: 4 (over y).
Axes of the slice: x: 4, y: 4, z: 8, core: 2. Of those that a mesh axis runs over, the one named last changes fastest.
Arguments:
- stream: bfloat16 [24576, 2048], P(('sp', 'tp')), may hold values from -6 to 6
- query_narrow: bfloat16 [24576, 512], P('sp', 'tp'), may hold values from -6 to 6
- key_narrow: bfloat16 [24576, 512], P('sp', 'tp'), may hold values from -6.5 to 6.5
- query_wide: bfloat16 [24576, 1024], P('sp', 'tp'), may hold values from -6 to 6
- key_wide: bfloat16 [24576, 1024], P('sp', 'tp'), may hold values from -6.5 to 6.5
- values: bfloat16 [24576, 2, 1024], P('sp', None, 'tp'), may hold values from -6 to 6
- out_gate: bfloat16 [24576, 2, 1024], P('sp', None, 'tp'), may hold values from -6 to 6
- out_weight: bfloat16 [2, 1024, 2048], P(None, 'tp'), may hold values from -0.125 to 0.125
- norm_gain: float32 [2048], replicated, may hold values from 0.1 to 1.9
- mlp_gate: bfloat16 [2048, 5632], P('sp', 'tp'), may hold values from -0.125 to 0.125
- mlp_up: bfloat16 [2048, 5632], P('sp', 'tp'), may hold values from -0.125 to 0.125
- mlp_down: bfloat16 [5632, 2048], P('tp', 'sp'), may hold values from -0.15625 to 0.15625
- log_decay: float32 [2, 2, 8], P(None, None, 'tp'), as said below
Outputs:
- layer_out: bfloat16 [24576, 2048], P(('sp', 'tp'))
The draws below stay inside these ranges and needn't reach their ends.
Inputs may be any that keep to these rules, and one draw needn't show every extreme that they name: `log_decay`: every entry is negative, with magnitude at least 0.5 / 24576.
All inputs are finite; a program needn't handle non-finite values.
Results may differ from the reference program's by a relative error of at most 0.013.
Values may be sent and summed in bfloat16 or wider, within the bound.
No kernel may reach another device: no remote copies, remote signals or barrier semaphores. Data moves between devices by JAX's collectives and lax.ppermute only.
A program may use at most 128 MiB of HBM per device.

```python
import jax
import jax.numpy as jnp
from jax import lax

D = 2048
FF = 5632
HG = 8
KA = 64
KB = 128
DV = 128
BLOCK = 128
TOK_DEV = 384
TOKENS = 24576
N_SP = 64


def draw_log_decay(key, part):
    slow_rates = jnp.exp(jax.random.uniform(jax.random.fold_in(key, 11), (2, 2, HG), jnp.float32, jnp.log(0.5), jnp.log(2.3))) / TOKENS
    fast_rates = jnp.exp(jax.random.uniform(jax.random.fold_in(key, 12), (2, 2, HG), jnp.float32, jnp.log(0.01), jnp.log(1.0 / 30.0)))
    forward_rank = jax.random.permutation(jax.random.fold_in(key, 13), 2 * HG)
    backward_rank = jax.random.permutation(jax.random.fold_in(key, 14), 2 * HG)
    ranking = jnp.stack([forward_rank, backward_rank]).reshape(2, 2, HG)
    chosen = jnp.where(ranking < HG, fast_rates, slow_rates)
    return -chosen


def steady_keys(key, head_size):
    result = jnp.clip(jax.random.normal(jax.random.fold_in(key, 1), (TOKENS, HG, head_size), jnp.float32), -6.0, 6.0)
    return result.reshape(TOKENS, HG * head_size).astype(jnp.bfloat16)


def draw_key_narrow(key, part):
    return steady_keys(jax.random.fold_in(key, 21), KA)


def draw_key_wide(key, part):
    return steady_keys(jax.random.fold_in(key, 31), KB)


def draw_values(key, part):
    base_key = jax.random.fold_in(key, 41)
    result = jnp.clip(jax.random.normal(jax.random.fold_in(base_key, 1), (TOKENS, 2, HG * DV), jnp.float32), -6.0, 6.0)
    return result.astype(jnp.bfloat16)


def steps_of(stream_key, dims, shards, low, high):
    factor_of, own = 1.0, jax.random.fold_in(stream_key, 6)
    for axis_at, parts in shards:
        steps = jnp.exp(jax.random.uniform(jax.random.fold_in(own, axis_at), (parts,), jnp.float32, low / len(shards), high / len(shards)))
        factor_of = factor_of * jnp.repeat(steps, dims[axis_at] // parts).reshape([-1 if axis == axis_at else 1 for axis in range(len(dims))])
    return factor_of


def normal_values(key, dims, spread, reach, cuts=(), kind=jnp.bfloat16):
    entries = jax.random.normal(key, dims, jnp.float32) * spread
    if len(cuts) > 0:
        entries = steps_of(key, dims, cuts, -0.22, 0.18) * entries
    return jnp.clip(entries, min=-reach, max=reach).astype(kind)


def setup_inputs(seed: int = 0) -> dict:
    keys = jax.random.split(jax.random.key(seed), 14)
    return {
        "stream": normal_values(keys[0], (TOKENS, D), 1.0, 6.0, ((0, 256),)),
        "query_narrow": normal_values(keys[1], (TOKENS, HG * KA), 1.0, 6.0, ((0, 64), (1, 4))),
        "key_narrow": draw_key_narrow(jax.random.fold_in(keys[13], 71), 0),
        "query_wide": normal_values(keys[3], (TOKENS, HG * KB), 1.0, 6.0, ((0, 64), (1, 4))),
        "key_wide": draw_key_wide(jax.random.fold_in(keys[13], 71), 0),
        "values": draw_values(jax.random.fold_in(keys[13], 71), 0),
        "out_gate": normal_values(keys[6], (TOKENS, 2, HG * DV), 1.0, 6.0, ((0, 64), (2, 4))),
        "out_weight": normal_values(keys[7], (2, HG * DV, D), (2 * HG * DV) ** -0.5, 0.125, ((1, 4),)),
        "norm_gain": jnp.clip(1.0 + 0.18 * jax.random.normal(keys[8], (D,), jnp.float32), 0.1, 1.9),
        "mlp_gate": normal_values(keys[9], (D, FF), D ** -0.5, 0.125, ((0, 64), (1, 4))),
        "mlp_up": normal_values(keys[10], (D, FF), D ** -0.5, 0.125, ((0, 64), (1, 4))),
        "mlp_down": normal_values(keys[11], (FF, D), (FF // 4) ** -0.5, 0.15625, ((0, 4), (1, 64))),
        "log_decay": draw_log_decay(jax.random.fold_in(keys[13], 71), 0),
    }


NORM_EPSILON = 1e-06
ROPE_BASE = 10000.0

def rotate(block_in, positions):
    half_size = block_in.shape[-1] // 2
    frequencies = jnp.power(ROPE_BASE, -(jnp.arange(half_size, dtype=jnp.float32) / half_size))
    angles = positions[:, None] * frequencies[None, :]
    cosine = jnp.cos(angles)[:, None, :]
    sine_table = jnp.sin(angles)[:, None, :]
    first_half = block_in[..., :half_size]
    second_half = block_in[..., half_size:]
    return jnp.concatenate([first_half * cosine - second_half * sine_table, first_half * sine_table + second_half * cosine], -1)

def decay_tables(rate_fwd, rate_bwd, block_len):
    position = jnp.arange(block_len, dtype=jnp.float32)
    offset = position[:, None] - position[None, :]
    forward_part = jnp.exp(rate_fwd[:, None, None] * jnp.maximum(offset, 0.0)[None])
    backward_part = jnp.exp(rate_bwd[:, None, None] * jnp.maximum(-offset, 0.0)[None])
    inner = jnp.where(offset[None] > 0, forward_part, jnp.where(offset[None] < 0, backward_part, 2.0))
    keep_fwd = jnp.exp(rate_fwd[:, None] * (block_len - 1.0 - position)[None, :])
    keep_bwd = jnp.exp(rate_bwd[:, None] * position[None, :])
    reach_fwd = jnp.exp(rate_fwd[:, None] * (position + 1.0)[None, :])
    reach_bwd = jnp.exp(rate_bwd[:, None] * (block_len - position)[None, :])
    return (inner, keep_fwd, keep_bwd, reach_fwd, reach_bwd)

def head_gate(combined, gate_rows):
    mean_value = lax.optimization_barrier(jnp.mean(combined, -1, keepdims=True))
    centred = combined - mean_value
    variance = lax.optimization_barrier(jnp.mean(centred * centred, -1, keepdims=True))
    scaled = centred * lax.rsqrt(variance + NORM_EPSILON)
    gated = jax.nn.silu(gate_rows.astype(jnp.float32)).reshape(combined.shape) * scaled
    return gated.reshape(combined.shape[0], -1).astype(jnp.bfloat16)

def retention_group(query_rows, key_rows, value_rows, gate_rows, rate_fwd, rate_bwd):
    length = query_rows.shape[0]
    head_count = rate_fwd.shape[0]
    key_size = query_rows.shape[1] // head_count
    value_size = value_rows.shape[1] // head_count
    positions = jnp.arange(length, dtype=jnp.float32)
    query_rot = rotate(query_rows.astype(jnp.float32).reshape(length, head_count, key_size), positions).astype(jnp.bfloat16)
    key_rot = (rotate(key_rows.astype(jnp.float32).reshape(length, head_count, key_size), positions) * key_size ** (-0.5)).astype(jnp.bfloat16)
    block_count = length // BLOCK
    query_blk = query_rot.reshape(block_count, BLOCK, head_count, key_size)
    key_blk = key_rot.reshape(block_count, BLOCK, head_count, key_size)
    value_blk = value_rows.reshape(block_count, BLOCK, head_count, value_size)
    inner, keep_fwd, keep_bwd, reach_fwd, reach_bwd = decay_tables(rate_fwd, rate_bwd, BLOCK)
    span_fwd = jnp.exp(rate_fwd * BLOCK)[:, None, None]
    span_bwd = jnp.exp(rate_bwd * BLOCK)[:, None, None]
    highest_precision = lax.Precision.HIGHEST

    def carry_step(keep_factor, decay_reach, span):

        def step(running_state, blocks):
            query_block_rows, key_block_rows, value_block_rows = blocks
            carried_state = jnp.einsum('zdf,dfe->zde', query_block_rows.astype(jnp.float32) * decay_reach.T[:, :, None], running_state, precision=highest_precision)
            state_update = jnp.einsum('tmu,tme->mue', key_block_rows.astype(jnp.float32) * keep_factor.T[:, :, None], value_block_rows.astype(jnp.float32), precision=highest_precision)
            return (span * running_state + state_update, carried_state)
        return step
    start_state = jnp.zeros((head_count, key_size, value_size), jnp.float32)
    blocks_all = (query_blk, key_blk, value_blk)
    _, carried_fwd = lax.scan(carry_step(keep_fwd, reach_fwd, span_fwd), start_state, blocks_all)
    _, carried_bwd = lax.scan(carry_step(keep_bwd, reach_bwd, span_bwd), start_state, blocks_all, reverse=True)

    def inside(blocks):
        query_block_rows, key_block_rows, value_block_rows = blocks
        scores = jnp.einsum('thk,shk->hts', query_block_rows.astype(jnp.float32), key_block_rows.astype(jnp.float32), precision=highest_precision)
        weights = (scores * inner).astype(jnp.bfloat16)
        return jnp.einsum('hts,shv->thv', weights.astype(jnp.float32), value_block_rows.astype(jnp.float32), precision=highest_precision)
    local_terms = lax.map(inside, blocks_all)
    combined = (local_terms + carried_fwd + carried_bwd).reshape(length, head_count, value_size)
    return head_gate(combined, gate_rows)

def rms_scale(rows_in, gain):
    widened = rows_in.astype(jnp.float32)
    return (widened * lax.rsqrt(lax.optimization_barrier(jnp.mean(widened * widened, -1, keepdims=True)) + NORM_EPSILON) * gain).astype(jnp.bfloat16)

def reference(stream, query_narrow, key_narrow, query_wide, key_wide, values, out_gate, out_weight, norm_gain, mlp_gate, mlp_up, mlp_down, log_decay):
    narrow_out = retention_group(query_narrow, key_narrow, values[:, 0], out_gate[:, 0], log_decay[0, 0], log_decay[1, 0])
    wide_out = retention_group(query_wide, key_wide, values[:, 1], out_gate[:, 1], log_decay[0, 1], log_decay[1, 1])

    def layer_rows(pieces):
        stream_rows, narrow_rows, wide_rows = pieces
        projection = jnp.dot(narrow_rows, out_weight[0], preferred_element_type=jnp.float32) + jnp.dot(wide_rows, out_weight[1], preferred_element_type=jnp.float32)
        middle = (stream_rows.astype(jnp.float32) + projection).astype(jnp.bfloat16)
        normed = rms_scale(middle, norm_gain)
        gate_act = jnp.dot(normed, mlp_gate, preferred_element_type=jnp.float32)
        up_act = jnp.dot(normed, mlp_up, preferred_element_type=jnp.float32)
        hidden = (jax.nn.silu(gate_act) * up_act).astype(jnp.bfloat16)
        down = jnp.dot(hidden, mlp_down, preferred_element_type=jnp.float32)
        return (middle.astype(jnp.float32) + 0.5 * down).astype(jnp.bfloat16)
    result = lax.map(layer_rows, (stream.reshape(N_SP, TOK_DEV, D), narrow_out.reshape(N_SP, TOK_DEV, -1), wide_out.reshape(N_SP, TOK_DEV, -1)))
    return result.reshape(TOKENS, D)
```

```python
import jax
import jax.numpy as jnp
from jax import lax
from jax.experimental import pallas as pl
from jax.experimental.pallas import tpu as pltpu
from jax.sharding import Mesh
from jax.sharding import PartitionSpec as P

SP = ("sp_0", "sp_1", "sp_2")
SP_TP = ("sp_0", "sp_1", "sp_2", "tp")

BLOCK = 128
NORM_EPSILON = 1e-06
ROPE_BASE = 10000.0
f32, bf16 = jnp.float32, jnp.bfloat16


def angle_tables(length, first):
    positions = (first + jnp.arange(length, dtype=jnp.int32)).astype(f32)
    wide = jnp.power(ROPE_BASE, -(jnp.arange(64, dtype=f32) / 64))
    narrow = jnp.power(ROPE_BASE, -(jnp.arange(32, dtype=f32) / 32))
    angles = positions[:, None] * jnp.concatenate([wide, narrow, narrow])[None]
    return jnp.cos(angles), jnp.sin(angles)


def lanes(shape):
    return lax.broadcasted_iota(jnp.int32, shape, len(shape) - 1)


def rows(shape):
    return lax.broadcasted_iota(jnp.int32, shape, 0)


def turned_wide(u, cosine, sine):
    lane = lanes(u.shape)
    c = jnp.where(lane < 64, cosine, pltpu.roll(cosine, 64, 1))
    s = jnp.where(lane < 64, -sine, pltpu.roll(sine, 64, 1))
    return u * c + pltpu.roll(u, 64, 1) * s


def turned_narrow(u, cosine, sine):
    lane = lanes(u.shape)
    c = jnp.where(lane < 64, pltpu.roll(cosine, 64, 1), cosine)
    s = jnp.where(lane < 64, pltpu.roll(sine, 64, 1), sine)
    low = (lane & 32) == 0
    other = jnp.where(low, pltpu.roll(u, 96, 1), pltpu.roll(u, 32, 1))
    return u * c + other * jnp.where(low, -s, s)


def split(x):
    high = x.astype(bf16)
    return high, (x - high.astype(f32)).astype(bf16)


def nt(a, b):
    return lax.dot_general(a, b, (((1,), (1,)), ((), ())), preferred_element_type=f32)


def tn(a, b):
    return lax.dot_general(a, b, (((0,), (0,)), ((), ())), preferred_element_type=f32)


def nn(a, b):
    return jnp.dot(a, b, preferred_element_type=f32)


def state_kernel(ld, kn, kw, v0, v1, cosine, sine, state, krn, krw):
    length = kn.shape[0]
    c, s = cosine[...], sine[...]
    kr_n = (turned_narrow(kn[...].astype(f32), c, s) * 64**-0.5).astype(bf16)
    krn[...] = kr_n
    t = rows((length, 128)).astype(f32)
    for h in range(4):
        g, i = h // 2, h % 2
        f, b = ld[g * 2 + i], ld[4 + g * 2 + i]
        if g == 0:
            kr = kr_n
        else:
            kr = (turned_wide(kw[:, i * 128 : (i + 1) * 128].astype(f32), c, s) * 128**-0.5).astype(bf16)
            krw[:, i * 128 : (i + 1) * 128] = kr
        v = (v0 if g == 0 else v1)[:, i * 128 : (i + 1) * 128].astype(f32)
        scaled = jnp.concatenate([v * jnp.exp(f * (length - 1.0 - t)), v * jnp.exp(b * t)], 1)
        high, low = split(scaled)
        total = tn(kr, high) + tn(kr, low)
        for d in range(2):
            part = total[:, d * 128 : (d + 1) * 128]
            if g == 0:
                state[:, d, i, :] = part[i * 64 : (i + 1) * 64]
            else:
                state[:, d, 2 + 2 * i, :] = part[:64]
                state[:, d, 3 + 2 * i, :] = part[64:]
    for d in range(2):
        for r in (6, 7):
            state[:, d, r, :] = jnp.zeros((64, 128), f32)


def inside_kernel(ld, qn, qw, krn, krw, v0, v1, cosine, sine, qrn, qrw, inside):
    length = qn.shape[0]
    c, s = cosine[...], sine[...]
    qr_n = turned_narrow(qn[...].astype(f32), c, s).astype(bf16)
    qrn[...] = qr_n
    lag = (rows((length, length)) - lanes((length, length))).astype(f32)
    away = jnp.abs(lag)
    for h in range(4):
        g, i = h // 2, h % 2
        f, b = ld[g * 2 + i], ld[4 + g * 2 + i]
        if g == 0:
            qr = jnp.where((lanes(qr_n.shape) // 64) == i, qr_n, jnp.zeros_like(qr_n))
            kr = krn[...]
        else:
            qr = turned_wide(qw[:, i * 128 : (i + 1) * 128].astype(f32), c, s).astype(bf16)
            qrw[:, i * 128 : (i + 1) * 128] = qr
            kr = krw[:, i * 128 : (i + 1) * 128]
        weight = jnp.where(lag == 0, 2.0, jnp.exp(jnp.where(lag > 0, f, b) * away))
        a = (nt(qr, kr) * weight).astype(bf16)
        v = (v0 if g == 0 else v1)[:, i * 128 : (i + 1) * 128]
        inside[:, h * 128 : (h + 1) * 128] = nn(a, v)


def finish_kernel(ld, qrn, qrw, inside, enter, g0, g1, weight, out):
    length = qrn.shape[0]
    t = rows((length, 128)).astype(f32)
    total = None
    for h in range(4):
        g, i = h // 2, h % 2
        f, b = ld[g * 2 + i], ld[4 + g * 2 + i]
        if g == 0:
            q = qrn[...]
            q = jnp.where((lanes(q.shape) // 64) == i, q, jnp.zeros_like(q))
            e = [jnp.concatenate([enter[:, d, i, :]] * 2, 0) for d in range(2)]
        else:
            q = qrw[:, i * 128 : (i + 1) * 128]
            e = [jnp.concatenate([enter[:, d, 2 + 2 * i, :], enter[:, d, 3 + 2 * i, :]], 0) for d in range(2)]
        high, low = split(jnp.concatenate(e, 1))
        carried = nn(q, high) + nn(q, low)
        ret = (
            inside[:, h * 128 : (h + 1) * 128]
            + carried[:, :128] * jnp.exp(f * (t + 1.0))
            + carried[:, 128:] * jnp.exp(b * (length - t))
        )
        mean = jnp.mean(ret, -1, keepdims=True)
        centred = ret - mean
        variance = jnp.mean(centred * centred, -1, keepdims=True)
        gate = (g0 if g == 0 else g1)[:, i * 128 : (i + 1) * 128].astype(f32)
        y = (gate * jax.nn.sigmoid(gate) * (centred * lax.rsqrt(variance + NORM_EPSILON))).astype(bf16)
        part = nn(y, weight[g, i * 128 : (i + 1) * 128, :])
        total = part if total is None else total + part
    out[...] = total.astype(bf16)


def scan_kernel(ld, x, out):
    r = rows((8, 128))

    def factor(base):
        rate = jnp.full((8, 128), ld[base + 3], f32)
        rate = jnp.where(r < 4, ld[base + 2], rate)
        rate = jnp.where(r == 1, ld[base + 1], rate)
        rate = jnp.where(r == 0, ld[base], rate)
        return jnp.exp(rate * 384.0)

    n = x.shape[0]
    forward, backward = factor(0), factor(4)
    acc = jnp.zeros((8, 128), f32)
    for k in range(n):
        out[k, 0] = acc
        acc = acc * forward + x[k, 0]
    acc = jnp.zeros((8, 128), f32)
    for k in reversed(range(n)):
        out[k, 1] = acc
        acc = acc * backward + x[k, 1]


SM = pl.BlockSpec(memory_space=pltpu.SMEM)
VM = pl.BlockSpec(memory_space=pltpu.VMEM)


def call(kernel, n_in, outs, name):
    return pl.pallas_call(
        kernel,
        in_specs=[SM] + [VM] * n_in,
        out_specs=jax.tree.map(lambda _: VM, outs),
        out_shape=outs,
        name=name,
        compiler_params=pltpu.CompilerParams(vmem_limit_bytes=40 * 2**20),
    )


def shape(*s, dtype=f32):
    return jax.ShapeDtypeStruct(s, dtype)


def rms_scale(rows_in, gain):
    widened = rows_in.astype(f32)
    return (
        widened * lax.rsqrt(jnp.mean(widened * widened, -1, keepdims=True) + NORM_EPSILON) * gain
    ).astype(bf16)


def exchanged(x, axis):
    return lax.all_to_all(x, axis, 0, 0, tiled=True)


def body(
    stream,
    query_narrow,
    key_narrow,
    query_wide,
    key_wide,
    values,
    out_gate,
    out_weight,
    norm_gain,
    mlp_gate,
    mlp_up,
    mlp_down,
    log_decay,
):
    length = query_narrow.shape[0]
    hidden_units = mlp_gate.shape[1]
    shards = lax.all_gather(jnp.concatenate([mlp_gate, mlp_up, mlp_down.T], 1), SP, axis=0, tiled=True)
    full_gate = shards[:, :hidden_units]
    full_up = shards[:, hidden_units : 2 * hidden_units]
    full_down = shards[:, 2 * hidden_units :]
    rates = log_decay.reshape(8)
    cosine, sine = angle_tables(length, lax.axis_index(SP) * length)
    v0, v1 = values[:, 0], values[:, 1]
    g0, g1 = out_gate[:, 0], out_gate[:, 1]
    n_rows, w_rows = shape(length, 128, dtype=bf16), shape(length, 256, dtype=bf16)
    states = shape(64, 2, 8, 128)
    state, krn, krw = call(state_kernel, 6, (states, n_rows, w_rows), "state")(
        rates, key_narrow, key_wide, v0, v1, cosine, sine
    )
    qrn, qrw, inside = call(inside_kernel, 8, (n_rows, w_rows, shape(length, 512)), "inside")(
        rates, query_narrow, query_wide, krn, krw, v0, v1, cosine, sine
    )
    enter = exchanged(call(scan_kernel, 1, states, "scan")(rates, exchanged(state, SP)), SP)
    proj = call(finish_kernel, 7, shape(length, 2048, dtype=bf16), "finish")(
        rates, qrn, qrw, inside, enter, g0, g1, out_weight
    )
    n_tp = lax.axis_size("tp")
    tiles = (n_tp, length // n_tp, proj.shape[1])
    proj_rows = jnp.sum(exchanged(proj.reshape(tiles), "tp").astype(f32), axis=0)
    middle = (stream.astype(f32) + proj_rows).astype(bf16)
    normed = exchanged(jnp.broadcast_to(rms_scale(middle, norm_gain)[None], tiles), "tp").reshape(length, -1)
    gate_act = jnp.dot(normed, full_gate, preferred_element_type=f32)
    up_act = jnp.dot(normed, full_up, preferred_element_type=f32)
    hidden = (jax.nn.silu(gate_act) * up_act).astype(bf16)
    down = nt(hidden, full_down).astype(bf16)
    down_rows = jnp.sum(exchanged(down.reshape(tiles), "tp").astype(f32), axis=0)
    return (middle.astype(f32) + 0.5 * down_rows).astype(bf16)


def solution(mesh):
    finer = Mesh(mesh.devices.reshape(8, 4, 2, mesh.shape["tp"]), ("sp_0", "sp_1", "sp_2", "tp"))
    return jax.shard_map(
        body,
        mesh=finer,
        in_specs=(
            P(SP_TP, None),
            P(SP, "tp"),
            P(SP, "tp"),
            P(SP, "tp"),
            P(SP, "tp"),
            P(SP, None, "tp"),
            P(SP, None, "tp"),
            P(None, "tp", None),
            P(),
            P(SP, "tp"),
            P(SP, "tp"),
            P("tp", SP),
            P(None, None, "tp"),
        ),
        out_specs=P(SP_TP, None),
        check_vma=False,
    )
```

```python
import jax
import jax.numpy as jnp
from jax import lax
from jax.experimental import pallas as pl
from jax.experimental.pallas import tpu as pltpu
from jax.sharding import Mesh
from jax.sharding import PartitionSpec as P

SP = ("sp_0", "sp_1", "sp_2")
SP_TP = ("sp_0", "sp_1", "sp_2", "tp")

BLOCK = 128
NORM_EPSILON = 1e-06
ROPE_BASE = 10000.0
f32, bf16 = jnp.float32, jnp.bfloat16


def angle_tables(length, first):
    positions = (first + jnp.arange(length, dtype=jnp.int32)).astype(f32)
    wide = jnp.power(ROPE_BASE, -(jnp.arange(64, dtype=f32) / 64))
    narrow = jnp.power(ROPE_BASE, -(jnp.arange(32, dtype=f32) / 32))
    angles = positions[:, None] * jnp.concatenate([wide, narrow, narrow])[None]
    return jnp.cos(angles), jnp.sin(angles)


def lanes(shape):
    return lax.broadcasted_iota(jnp.int32, shape, len(shape) - 1)


def rows(shape):
    return lax.broadcasted_iota(jnp.int32, shape, 0)


def turned_wide(u, cosine, sine):
    lane = lanes(u.shape)
    c = jnp.where(lane < 64, cosine, pltpu.roll(cosine, 64, 1))
    s = jnp.where(lane < 64, -sine, pltpu.roll(sine, 64, 1))
    return u * c + pltpu.roll(u, 64, 1) * s


def turned_narrow(u, cosine, sine):
    lane = lanes(u.shape)
    c = jnp.where(lane < 64, pltpu.roll(cosine, 64, 1), cosine)
    s = jnp.where(lane < 64, pltpu.roll(sine, 64, 1), sine)
    low = (lane & 32) == 0
    other = jnp.where(low, pltpu.roll(u, 96, 1), pltpu.roll(u, 32, 1))
    return u * c + other * jnp.where(low, -s, s)


def split(x):
    high = x.astype(bf16)
    return high, (x - high.astype(f32)).astype(bf16)


def nt(a, b):
    return lax.dot_general(a, b, (((1,), (1,)), ((), ())), preferred_element_type=f32)


def tn(a, b):
    return lax.dot_general(a, b, (((0,), (0,)), ((), ())), preferred_element_type=f32)


def nn(a, b):
    return jnp.dot(a, b, preferred_element_type=f32)


STATE = bf16


def turned_all(narrow, wide, cosine, sine, scales):
    c, s = cosine[...], sine[...]
    parts = [turned_narrow(narrow[...].astype(f32), c, s) * scales[0]]
    for i in range(2):
        parts.append(turned_wide(wide[:, i * 128 : (i + 1) * 128].astype(f32), c, s) * scales[1])
    return [p.astype(bf16) for p in parts]


def of_head(parts, h):
    if h >= 2:
        return parts[h - 1]
    return jnp.where((lanes(parts[0].shape) // 64) == h, parts[0], jnp.zeros_like(parts[0]))


KEY_SCALES = (64**-0.5, 128**-0.5)


def state_kernel(ld, kn, kw, v0, v1, cosine, sine, out, state):
    length = kn.shape[0]
    keys = turned_all(kn, kw, cosine, sine, KEY_SCALES)
    t = rows((length, 128)).astype(f32)
    for h in range(4):
        g, i = h // 2, h % 2
        f, b = ld[g * 2 + i], ld[4 + g * 2 + i]
        v = (v0 if g == 0 else v1)[:, i * 128 : (i + 1) * 128].astype(f32)
        scaled = jnp.concatenate([v * jnp.exp(f * (length - 1.0 - t)), v * jnp.exp(b * t)], 1)
        high, low = split(scaled)
        kr = keys[0] if g == 0 else keys[1 + i]
        total = tn(kr, high) + tn(kr, low)
        for d in range(2):
            part = total[:, d * 128 : (d + 1) * 128]
            if g == 0:
                state[:, d, i, :] = part[i * 64 : (i + 1) * 64]
            else:
                state[:, d, 2 + 2 * i, :] = part[:64]
                state[:, d, 3 + 2 * i, :] = part[64:]
    for d in range(2):
        for r in (6, 7):
            state[:, d, r, :] = jnp.zeros((64, 128), f32)
    out[...] = state[...].astype(STATE)


def inside_kernel(ld, qn, qw, kn, kw, v0, v1, cosine, sine, turned, inside):
    length = qn.shape[0]
    queries = turned_all(qn, qw, cosine, sine, (1.0, 1.0))
    keys = turned_all(kn, kw, cosine, sine, KEY_SCALES)
    for k in range(3):
        turned[:, k * 128 : (k + 1) * 128] = queries[k]
    lag = (rows((length, length)) - lanes((length, length))).astype(f32)
    away = jnp.abs(lag)
    for h in range(4):
        g, i = h // 2, h % 2
        f, b = ld[g * 2 + i], ld[4 + g * 2 + i]
        kr = keys[0] if g == 0 else keys[1 + i]
        weight = jnp.where(lag == 0, 2.0, jnp.exp(jnp.where(lag > 0, f, b) * away))
        a = (nt(of_head(queries, h), kr) * weight).astype(bf16)
        v = (v0 if g == 0 else v1)[:, i * 128 : (i + 1) * 128]
        inside[:, h * 128 : (h + 1) * 128] = nn(a, v)


def finish_kernel(ld, turned_in, inside_in, enter_in, g0, g1, out, turned, inside, enter, sems):
    copies = [
        pltpu.make_async_copy(turned_in, turned, sems.at[0]),
        pltpu.make_async_copy(inside_in, inside, sems.at[1]),
    ]
    for copy in copies:
        copy.start()
    enter[...] = enter_in[...].astype(f32)
    length = turned.shape[0]
    t = rows((length, 128)).astype(f32)
    states = []
    for h in range(4):
        g, i = h // 2, h % 2
        if g == 0:
            e = [jnp.concatenate([enter[:, d, i, :]] * 2, 0) for d in range(2)]
        else:
            e = [jnp.concatenate([enter[:, d, 2 + 2 * i, :], enter[:, d, 3 + 2 * i, :]], 0) for d in range(2)]
        states.append(split(jnp.concatenate(e, 1)))
    for copy in copies:
        copy.wait()
    queries = [turned[:, k * 128 : (k + 1) * 128] for k in range(3)]
    for h in range(4):
        g, i = h // 2, h % 2
        f, b = ld[g * 2 + i], ld[4 + g * 2 + i]
        q = of_head(queries, h)
        high, low = states[h]
        carried = nn(q, high) + nn(q, low)
        ret = (
            inside[:, h * 128 : (h + 1) * 128]
            + carried[:, :128] * jnp.exp(f * (t + 1.0))
            + carried[:, 128:] * jnp.exp(b * (length - t))
        )
        mean = jnp.mean(ret, -1, keepdims=True)
        centred = ret - mean
        variance = jnp.mean(centred * centred, -1, keepdims=True)
        gate = (g0 if g == 0 else g1)[:, i * 128 : (i + 1) * 128].astype(f32)
        y = gate * jax.nn.sigmoid(gate) * (centred * lax.rsqrt(variance + NORM_EPSILON))
        out[:, h * 128 : (h + 1) * 128] = y.astype(bf16)


def scan_kernel(ld, x, out):
    r = rows((8, 128))

    def factor(base):
        rate = jnp.full((8, 128), ld[base + 3], f32)
        rate = jnp.where(r < 4, ld[base + 2], rate)
        rate = jnp.where(r == 1, ld[base + 1], rate)
        rate = jnp.where(r == 0, ld[base], rate)
        return jnp.exp(rate * 384.0)

    n = x.shape[0]
    forward, backward = factor(0), factor(4)
    acc = jnp.zeros((8, 128), f32)
    for k in range(n):
        out[k, 0] = acc.astype(STATE)
        acc = acc * forward + x[k, 0].astype(f32)
    acc = jnp.zeros((8, 128), f32)
    for k in reversed(range(n)):
        out[k, 1] = acc.astype(STATE)
        acc = acc * backward + x[k, 1].astype(f32)


def proj_kernel(place, y, stream, gain, own, *refs):
    others, (middle, normed, blocks, sems) = refs[:6], refs[6:]
    sources = [own.at[0], own.at[1], *others]
    copies = [pltpu.make_async_copy(s, blocks.at[k], sems.at[k]) for k, s in enumerate(sources)]
    for copy in copies:
        copy.start()
    tp, core = place[0], place[1]
    total = stream[...].astype(f32)
    for k, copy in enumerate(copies):
        if k < 2:
            rows_in = y[tp, :, k * 256 : (k + 1) * 256]
        else:
            piece = y[(tp + 4 - (k // 2)) % 4]
            first, second = (core, 1 - core) if k % 2 == 0 else (1 - core, core)
            rows_in = jnp.where(first == 0, piece[:, :256], piece[:, 256:])
        copy.wait()
        part = nn(rows_in, blocks[k])
        proj = part if k == 0 else proj + part
    mid = (total + proj).astype(bf16)
    middle[...] = mid
    wide = mid.astype(f32)
    scale = lax.rsqrt(jnp.mean(wide * wide, -1, keepdims=True) + NORM_EPSILON)
    normed[...] = (wide * scale * gain[...]).astype(bf16)


SM = pl.BlockSpec(memory_space=pltpu.SMEM)
VM = pl.BlockSpec(memory_space=pltpu.VMEM)
HB = pl.BlockSpec(memory_space=pltpu.HBM)


def call(kernel, in_specs, outs, name, scratch=()):
    return pl.pallas_call(
        kernel,
        in_specs=in_specs,
        out_specs=jax.tree.map(lambda _: VM, outs),
        out_shape=outs,
        scratch_shapes=scratch,
        name=name,
        compiler_params=pltpu.CompilerParams(vmem_limit_bytes=40 * 2**20),
    )


def shape(*s, dtype=f32):
    return jax.ShapeDtypeStruct(s, dtype)


def exchanged(x, axis):
    return lax.all_to_all(x, axis, 0, 0, tiled=True)


def after(x, token):
    return lax.optimization_barrier((x, token))[0]


def shifted(x, by):
    n = lax.axis_size("tp")
    return lax.ppermute(x, "tp", [(k, (k + by) % n) for k in range(n)])


def body(
    stream,
    query_narrow,
    key_narrow,
    query_wide,
    key_wide,
    values,
    out_gate,
    out_weight,
    norm_gain,
    mlp_gate,
    mlp_up,
    mlp_down,
    log_decay,
):
    length, width = query_narrow.shape[0], stream.shape[1]
    hidden_units = mlp_gate.shape[1]
    shards = lax.all_gather(jnp.concatenate([mlp_gate, mlp_up], 1), SP, axis=0, tiled=True)
    full_gate, full_up = shards[:, :hidden_units], shards[:, hidden_units:]
    full_down = lax.all_gather(mlp_down.T, SP, axis=0, tiled=True)

    rates = log_decay.reshape(8)
    cosine, sine = angle_tables(length, lax.axis_index(SP) * length)
    v0, v1 = values[:, 0], values[:, 1]
    g0, g1 = out_gate[:, 0], out_gate[:, 1]
    states = shape(64, 2, 8, 128, dtype=STATE)
    state = call(state_kernel, [SM] + [VM] * 6, states, "state", (pltpu.VMEM((64, 2, 8, 128), f32),))(
        rates, key_narrow, key_wide, v0, v1, cosine, sine
    )
    core = lax.axis_index("sp_2")
    half = lax.dynamic_index_in_dim(after(out_weight, state), core, 0, keepdims=False)
    same = [shifted(half, s) for s in (1, 2, 3)]
    turned, inside = call(
        inside_kernel, [SM] + [VM] * 8, (shape(length, 384, dtype=bf16), shape(length, 512)), "inside"
    )(rates, query_narrow, query_wide, key_narrow, key_wide, v0, v1, cosine, sine)
    arrived = exchanged(state, SP)
    enter = call(scan_kernel, [SM, VM], states, "scan")(rates, arrived)
    enter = exchanged(enter, SP)
    y = call(
        finish_kernel,
        [SM, HB, HB, VM, VM, VM],
        shape(length, 512, dtype=bf16),
        "finish",
        (pltpu.VMEM((length, 384), bf16), pltpu.VMEM((length, 512), f32), pltpu.VMEM((64, 2, 8, 128), f32), pltpu.SemaphoreType.DMA((2,))),
    )(rates, turned, inside, enter, g0, g1)
    other = [lax.ppermute(after(w, y), "sp_2", [(0, 1), (1, 0)]) for w in same]
    n_tp = lax.axis_size("tp")
    y = exchanged(y.reshape(n_tp, length // n_tp, 512), "tp")
    own = shape(length // n_tp, width, dtype=bf16)
    place = jnp.stack([lax.axis_index("tp"), core]).astype(jnp.int32)
    pieces = [w for pair in zip(same, other) for w in pair]
    middle, normed = call(
        proj_kernel,
        [SM, VM, VM, VM] + [HB] * 7,
        (own, own),
        "proj",
        (pltpu.VMEM((8, 256, width), bf16), pltpu.SemaphoreType.DMA((8,))),
    )(place, y, stream, norm_gain[None], out_weight, *pieces)

    def mixed(x):
        gate_act = jnp.dot(x, full_gate, preferred_element_type=f32)
        up_act = jnp.dot(x, full_up, preferred_element_type=f32)
        return (jax.nn.silu(gate_act) * up_act).astype(bf16)

    near = mixed(jnp.concatenate([shifted(normed, 1), shifted(normed, 3)], 0))
    far = mixed(jnp.concatenate([normed, shifted(normed, 2)], 0))
    near, far, full_down = lax.optimization_barrier((near, far, full_down))
    near = nt(near, full_down).astype(bf16)
    far = nt(far, full_down).astype(bf16)
    n = length // n_tp
    total = far[:n].astype(f32) + shifted(far[n:], 2).astype(f32)
    total = total + shifted(near[:n], 3).astype(f32) + shifted(near[n:], 1).astype(f32)
    return (middle.astype(f32) + 0.5 * total).astype(bf16)


def solution(mesh):
    finer = Mesh(mesh.devices.reshape(8, 4, 2, mesh.shape["tp"]), ("sp_0", "sp_1", "sp_2", "tp"))
    return jax.shard_map(
        body,
        mesh=finer,
        in_specs=(
            P(SP_TP, None),
            P(SP, "tp"),
            P(SP, "tp"),
            P(SP, "tp"),
            P(SP, "tp"),
            P(SP, None, "tp"),
            P(SP, None, "tp"),
            P(None, "tp", None),
            P(),
            P(SP, "tp"),
            P(SP, "tp"),
            P("tp", SP),
            P(None, None, "tp"),
        ),
        out_specs=P(SP_TP, None),
        check_vma=False,
    )
```

```python
import jax
import jax.numpy as jnp
from jax import lax
from jax.experimental import pallas as pl
from jax.experimental.pallas import tpu as pltpu
from jax.sharding import Mesh
from jax.sharding import PartitionSpec as P


SP = ("sp_0", "sp_1", "sp_2")
SP_TP = ("sp_0", "sp_1", "sp_2", "tp")

NORM_EPSILON = 1e-06
ROPE_BASE = 10000.0
f32, bf16 = jnp.float32, jnp.bfloat16


def angle_tables(length, first):
    positions = (first + jnp.arange(length, dtype=jnp.int32)).astype(f32)
    wide = jnp.power(ROPE_BASE, -(jnp.arange(64, dtype=f32) / 64))
    narrow = jnp.power(ROPE_BASE, -(jnp.arange(32, dtype=f32) / 32))
    angles = positions[:, None] * jnp.concatenate([wide, narrow, narrow])[None]
    return jnp.cos(angles), jnp.sin(angles)


def lanes(shape):
    return lax.broadcasted_iota(jnp.int32, shape, len(shape) - 1)


def rows(shape):
    return lax.broadcasted_iota(jnp.int32, shape, 0)


def turned_wide(u, cosine, sine):
    lane = lanes(u.shape)
    c = jnp.where(lane < 64, cosine, pltpu.roll(cosine, 64, 1))
    s = jnp.where(lane < 64, -sine, pltpu.roll(sine, 64, 1))
    return u * c + pltpu.roll(u, 64, 1) * s


def turned_narrow(u, cosine, sine):
    lane = lanes(u.shape)
    c = jnp.where(lane < 64, pltpu.roll(cosine, 64, 1), cosine)
    s = jnp.where(lane < 64, pltpu.roll(sine, 64, 1), sine)
    low = (lane & 32) == 0
    other = jnp.where(low, pltpu.roll(u, 96, 1), pltpu.roll(u, 32, 1))
    return u * c + other * jnp.where(low, -s, s)


def split(x):
    high = x.astype(bf16)
    return high, (x - high.astype(f32)).astype(bf16)


def nt(a, b):
    return lax.dot_general(a, b, (((1,), (1,)), ((), ())), preferred_element_type=f32)


def tn(a, b):
    return lax.dot_general(a, b, (((0,), (0,)), ((), ())), preferred_element_type=f32)


def nn(a, b):
    return jnp.dot(a, b, preferred_element_type=f32)


STATE = bf16


def turned_all(narrow, wide, cosine, sine, scales):
    c, s = cosine[...], sine[...]
    parts = [turned_narrow(narrow[...].astype(f32), c, s) * scales[0]]
    for i in range(2):
        parts.append(turned_wide(wide[:, i * 128 : (i + 1) * 128].astype(f32), c, s) * scales[1])
    return [p.astype(bf16) for p in parts]


def of_head(parts, h):
    if h >= 2:
        return parts[h - 1]
    return jnp.where((lanes(parts[0].shape) // 64) == h, parts[0], jnp.zeros_like(parts[0]))


KEY_SCALES = (64**-0.5, 128**-0.5)


def state_kernel(ld, kn, kw, values, cosine, sine, out, state):
    length = kn.shape[0]
    keys = turned_all(kn, kw, cosine, sine, KEY_SCALES)
    t = rows((length, 128)).astype(f32)
    for h in range(4):
        g, i = h // 2, h % 2
        f, b = ld[0, g, i], ld[1, g, i]
        v = values[:, g, i * 128 : (i + 1) * 128].astype(f32)
        scaled = jnp.concatenate([v * jnp.exp(f * (length - 1.0 - t)), v * jnp.exp(b * t)], 1)
        high, low = split(scaled)
        kr = keys[0] if g == 0 else keys[1 + i]
        total = tn(kr, high) + tn(kr, low)
        for d in range(2):
            part = total[:, d * 128 : (d + 1) * 128]
            if g == 0:
                state[:, d, i, :] = part[i * 64 : (i + 1) * 64]
            else:
                state[:, d, 2 + 2 * i, :] = part[:64]
                state[:, d, 3 + 2 * i, :] = part[64:]
    for d in range(2):
        for r in (6, 7):
            state[:, d, r, :] = jnp.zeros((64, 128), f32)
    out[...] = state[...].astype(STATE)


def inside_kernel(ld, qn, qw, kn, kw, values, cosine, sine, turned_out, inside_out, turned, inside, sems):
    length = qn.shape[0]
    queries = turned_all(qn, qw, cosine, sine, (1.0, 1.0))
    keys = turned_all(kn, kw, cosine, sine, KEY_SCALES)
    for k in range(3):
        turned[:, k * 128 : (k + 1) * 128] = queries[k]
    turned_copy = pltpu.make_async_copy(turned, turned_out, sems.at[0])
    turned_copy.start()
    lag = (rows((length, length)) - lanes((length, length))).astype(f32)
    away = jnp.abs(lag)
    for h in range(4):
        g, i = h // 2, h % 2
        f, b = ld[0, g, i], ld[1, g, i]
        kr = keys[0] if g == 0 else keys[1 + i]
        weight = jnp.where(lag == 0, 2.0, jnp.exp(jnp.where(lag > 0, f, b) * away))
        a = (nt(of_head(queries, h), kr) * weight).astype(bf16)
        v = values[:, g, i * 128 : (i + 1) * 128]
        inside[:, h * 128 : (h + 1) * 128] = nn(a, v)
    inside_copy = pltpu.make_async_copy(inside, inside_out, sems.at[1])
    inside_copy.start()
    turned_copy.wait()
    inside_copy.wait()


def finish_kernel(ld, turned_in, inside_in, enter_in, gates, out, turned, inside, enter, sems):
    copies = [
        pltpu.make_async_copy(turned_in, turned, sems.at[0]),
        pltpu.make_async_copy(inside_in, inside, sems.at[1]),
    ]
    for copy in copies:
        copy.start()
    enter[...] = enter_in[...].astype(f32)
    length = turned.shape[0]
    t = rows((length, 128)).astype(f32)
    states = []
    for h in range(4):
        g, i = h // 2, h % 2
        if g == 0:
            e = [jnp.concatenate([enter[:, d, i, :]] * 2, 0) for d in range(2)]
        else:
            e = [jnp.concatenate([enter[:, d, 2 + 2 * i, :], enter[:, d, 3 + 2 * i, :]], 0) for d in range(2)]
        states.append(split(jnp.concatenate(e, 1)))
    for copy in copies:
        copy.wait()
    queries = [turned[:, k * 128 : (k + 1) * 128] for k in range(3)]
    for h in range(4):
        g, i = h // 2, h % 2
        f, b = ld[0, g, i], ld[1, g, i]
        q = of_head(queries, h)
        high, low = states[h]
        carried = nn(q, high) + nn(q, low)
        ret = (
            inside[:, h * 128 : (h + 1) * 128]
            + carried[:, :128] * jnp.exp(f * (t + 1.0))
            + carried[:, 128:] * jnp.exp(b * (length - t))
        )
        mean = jnp.mean(ret, -1, keepdims=True)
        centred = ret - mean
        variance = jnp.mean(centred * centred, -1, keepdims=True)
        gate = gates[:, g, i * 128 : (i + 1) * 128].astype(f32)
        y = gate * jax.nn.sigmoid(gate) * (centred * lax.rsqrt(variance + NORM_EPSILON))
        out[:, h * 128 : (h + 1) * 128] = y.astype(bf16)


def scan_kernel(ld, x, out):
    r = rows((8, 128))

    def factor(d):
        rate = jnp.full((8, 128), ld[d, 1, 1], f32)
        rate = jnp.where(r < 4, ld[d, 1, 0], rate)
        rate = jnp.where(r == 1, ld[d, 0, 1], rate)
        rate = jnp.where(r == 0, ld[d, 0, 0], rate)
        return jnp.exp(rate * 384.0)

    n = x.shape[0]
    forward, backward = factor(0), factor(1)
    acc = jnp.zeros((8, 128), f32)
    for k in range(n):
        out[k, 0] = acc.astype(STATE)
        acc = acc * forward + x[k, 0].astype(f32)
    acc = jnp.zeros((8, 128), f32)
    for k in reversed(range(n)):
        out[k, 1] = acc.astype(STATE)
        acc = acc * backward + x[k, 1].astype(f32)


def proj_kernel(place, y, stream, gain, own, *refs):
    others, (middle, normed, blocks, sems) = refs[:6], refs[6:]
    sources = [own.at[0], own.at[1], *others]
    copies = [pltpu.make_async_copy(s, blocks.at[k], sems.at[k]) for k, s in enumerate(sources)]
    for copy in copies:
        copy.start()
    tp, core = place[0], place[1]
    total = stream[...].astype(f32)
    for k, copy in enumerate(copies):
        if k < 2:
            rows_in = y[tp, :, k * 256 : (k + 1) * 256]
        else:
            piece = y[(tp + 4 - (k // 2)) % 4]
            first, _ = (core, 1 - core) if k % 2 == 0 else (1 - core, core)
            rows_in = jnp.where(first == 0, piece[:, :256], piece[:, 256:])
        copy.wait()
        part = nn(rows_in, blocks[k])
        proj = part if k == 0 else proj + part
    mid = (total + proj).astype(bf16)
    middle[...] = mid
    wide = mid.astype(f32)
    scale = lax.rsqrt(jnp.mean(wide * wide, -1, keepdims=True) + NORM_EPSILON)
    normed[...] = (wide * scale * gain[...]).astype(bf16)


SM = pl.BlockSpec(memory_space=pltpu.SMEM)
VM = pl.BlockSpec(memory_space=pltpu.VMEM)
HB = pl.BlockSpec(memory_space=pltpu.HBM)


def call(kernel, in_specs, outs, scratch=(), out_specs=None):
    return pl.pallas_call(
        kernel,
        in_specs=in_specs,
        out_specs=out_specs or jax.tree.map(lambda _: VM, outs),
        out_shape=outs,
        scratch_shapes=scratch,
        compiler_params=pltpu.CompilerParams(vmem_limit_bytes=40 * 2**20),
    )


def shape(*s, dtype=f32):
    return jax.ShapeDtypeStruct(s, dtype)


def exchanged(x, axis):
    return lax.all_to_all(x, axis, 0, 0, tiled=True)


def after(x, token):
    return lax.optimization_barrier((x, token))[0]


def shifted(x, by):
    n = lax.axis_size("tp")
    return lax.ppermute(x, "tp", [(k, (k + by) % n) for k in range(n)])


def body(
    stream,
    query_narrow,
    key_narrow,
    query_wide,
    key_wide,
    values,
    out_gate,
    out_weight,
    norm_gain,
    mlp_gate,
    mlp_up,
    mlp_down,
    log_decay,
):
    length, width = query_narrow.shape[0], stream.shape[1]
    hidden_units = mlp_gate.shape[1]
    shards = lax.all_gather(jnp.concatenate([mlp_gate, mlp_up, mlp_down.T], 1), SP, axis=0, tiled=True)
    full_gate, full_up, full_down = (shards[:, k * hidden_units : (k + 1) * hidden_units] for k in range(3))

    rates = log_decay
    cosine, sine = angle_tables(length, lax.axis_index(SP) * length)
    states = shape(64, 2, 8, 128, dtype=STATE)
    state = call(state_kernel, [SM] + [VM] * 5, states, (pltpu.VMEM((64, 2, 8, 128), f32),))(
        rates, key_narrow, key_wide, values, cosine, sine
    )
    core = lax.axis_index("sp_2")
    half = lax.dynamic_index_in_dim(after(out_weight, state), core, 0, keepdims=False)
    same = []
    for s in (1, 2, 3):
        same.append(shifted(half, s))
    kept = [((length, 384), bf16), ((length, 512), f32)]
    turned, inside = call(
        inside_kernel,
        [SM] + [VM] * 7,
        tuple(pltpu.HBM(*k) for k in kept),
        tuple(pltpu.VMEM(*k) for k in kept) + (pltpu.SemaphoreType.DMA((2,)),),
        (HB, HB),
    )(rates, query_narrow, query_wide, key_narrow, key_wide, values, cosine, sine)
    arrived = exchanged(state, SP)
    enter = call(scan_kernel, [SM, VM], states)(rates, arrived)
    enter = exchanged(enter, SP)
    y = call(
        finish_kernel,
        [SM, HB, HB, VM, VM],
        shape(length, 512, dtype=bf16),
        (pltpu.VMEM((length, 384), bf16), pltpu.VMEM((length, 512), f32), pltpu.VMEM((64, 2, 8, 128), f32), pltpu.SemaphoreType.DMA((2,))),
    )(rates, turned, inside, enter, out_gate)
    other = []
    for s in (1, 2, 3):
        other.append(lax.ppermute(after(same[s - 1], y), "sp_2", [(0, 1), (1, 0)]))
    n_tp = lax.axis_size("tp")
    y = exchanged(y.reshape(n_tp, length // n_tp, 512), "tp")
    own = shape(length // n_tp, width, dtype=bf16)
    place = jnp.stack([lax.axis_index("tp"), core]).astype(jnp.int32)
    pieces = [w for pair in zip(same, other) for w in pair]
    middle, normed = call(
        proj_kernel,
        [SM, VM, VM, VM] + [HB] * 7,
        (own, own),
        (pltpu.VMEM((8, 256, width), bf16), pltpu.SemaphoreType.DMA((8,))),
    )(place, y, stream, norm_gain[None], out_weight, *pieces)

    def mixed(x):
        gate_act = jnp.dot(x, full_gate, preferred_element_type=f32)
        up_act = jnp.dot(x, full_up, preferred_element_type=f32)
        return (jax.nn.silu(gate_act) * up_act).astype(bf16)

    near = mixed(jnp.concatenate([shifted(normed, 1), shifted(normed, 3)], 0))
    far = mixed(jnp.concatenate([normed, shifted(normed, 2)], 0))
    near = nt(near, full_down).astype(bf16)
    far = nt(far, full_down).astype(bf16)
    n = length // n_tp
    total = far[:n].astype(f32) + shifted(far[n:], 2).astype(f32)
    total = total + shifted(near[:n], 3).astype(f32) + shifted(near[n:], 1).astype(f32)
    return (middle.astype(f32) + 0.5 * total).astype(bf16)


def solution(mesh):
    finer = Mesh(mesh.devices.reshape(8, 4, 2, mesh.shape["tp"]), ("sp_0", "sp_1", "sp_2", "tp"))
    return jax.shard_map(
        body,
        mesh=finer,
        in_specs=(
            P(SP_TP, None),
            P(SP, "tp"),
            P(SP, "tp"),
            P(SP, "tp"),
            P(SP, "tp"),
            P(SP, None, "tp"),
            P(SP, None, "tp"),
            P(None, "tp", None),
            P(),
            P(SP, "tp"),
            P(SP, "tp"),
            P("tp", SP),
            P(None, None, "tp"),
        ),
        out_specs=P(SP_TP, None),
        check_vma=False,
    )
```

```python
import jax
import jax.numpy as jnp
from jax import lax
from jax.experimental import pallas as pl
from jax.experimental.pallas import tpu as pltpu
from jax.sharding import Mesh
from jax.sharding import PartitionSpec as P


SP = ("sp_0", "sp_1", "sp_2")
SP_TP = ("sp_0", "sp_1", "sp_2", "tp")

NORM_EPSILON = 1e-06
ROPE_BASE = 10000.0
f32, bf16 = jnp.float32, jnp.bfloat16


def angle_tables(length, first):
    positions = (first + jnp.arange(length, dtype=jnp.int32)).astype(f32)
    wide = jnp.power(ROPE_BASE, -(jnp.arange(64, dtype=f32) / 64))
    narrow = jnp.power(ROPE_BASE, -(jnp.arange(32, dtype=f32) / 32))
    angles = positions[:, None] * jnp.concatenate([wide, narrow, narrow])[None]
    return jnp.cos(angles), jnp.sin(angles)


def lanes(shape):
    return lax.broadcasted_iota(jnp.int32, shape, len(shape) - 1)


def rows(shape):
    return lax.broadcasted_iota(jnp.int32, shape, 0)


def turned_wide(u, cosine, sine):
    lane = lanes(u.shape)
    c = jnp.where(lane < 64, cosine, pltpu.roll(cosine, 64, 1))
    s = jnp.where(lane < 64, -sine, pltpu.roll(sine, 64, 1))
    return u * c + pltpu.roll(u, 64, 1) * s


def turned_narrow(u, cosine, sine):
    lane = lanes(u.shape)
    c = jnp.where(lane < 64, pltpu.roll(cosine, 64, 1), cosine)
    s = jnp.where(lane < 64, pltpu.roll(sine, 64, 1), sine)
    low = (lane & 32) == 0
    other = jnp.where(low, pltpu.roll(u, 96, 1), pltpu.roll(u, 32, 1))
    return u * c + other * jnp.where(low, -s, s)


def split(x):
    high = x.astype(bf16)
    return high, (x - high.astype(f32)).astype(bf16)


def nt(a, b):
    return lax.dot_general(a, b, (((1,), (1,)), ((), ())), preferred_element_type=f32)


def tn(a, b):
    return lax.dot_general(a, b, (((0,), (0,)), ((), ())), preferred_element_type=f32)


def nn(a, b):
    return jnp.dot(a, b, preferred_element_type=f32)


STATE = bf16
STAGES = 4


def turned_all(narrow, wide, cosine, sine, scales):
    c, s = cosine[...], sine[...]
    parts = [turned_narrow(narrow[...].astype(f32), c, s) * scales[0]]
    for i in range(2):
        parts.append(turned_wide(wide[:, i * 128 : (i + 1) * 128].astype(f32), c, s) * scales[1])
    return [p.astype(bf16) for p in parts]


def of_head(parts, h):
    if h >= 2:
        return parts[h - 1]
    return jnp.where((lanes(parts[0].shape) // 64) == h, parts[0], jnp.zeros_like(parts[0]))


KEY_SCALES = (64**-0.5, 128**-0.5)


def state_kernel(ld, kn, kw, v0, v1, cosine, sine, out, state):
    length = kn.shape[0]
    keys = turned_all(kn, kw, cosine, sine, KEY_SCALES)
    t = rows((length, 128)).astype(f32)
    for h in range(4):
        g, i = h // 2, h % 2
        f, b = ld[0, g, i], ld[1, g, i]
        v = (v0 if g == 0 else v1)[:, i * 128 : (i + 1) * 128].astype(f32)
        scaled = jnp.concatenate([v * jnp.exp(f * (length - 1.0 - t)), v * jnp.exp(b * t)], 1)
        high, low = split(scaled)
        kr = keys[0] if g == 0 else keys[1 + i]
        total = tn(kr, high) + tn(kr, low)
        for d in range(2):
            part = total[:, d * 128 : (d + 1) * 128]
            if g == 0:
                state[:, d, i, :] = part[i * 64 : (i + 1) * 64]
            else:
                state[:, d, 2 + 2 * i, :] = part[:64]
                state[:, d, 3 + 2 * i, :] = part[64:]
    for d in range(2):
        for r in (6, 7):
            state[:, d, r, :] = jnp.zeros((64, 128), f32)
    out[...] = state[...].astype(STATE)


def inside_kernel(ld, qn, qw, kn, kw, v0, v1, cosine, sine, turned_out, inside_out, turned, inside, sems):
    length = qn.shape[0]
    queries = turned_all(qn, qw, cosine, sine, (1.0, 1.0))
    keys = turned_all(kn, kw, cosine, sine, KEY_SCALES)
    for k in range(3):
        turned[:, k * 128 : (k + 1) * 128] = queries[k]
    turned_copy = pltpu.make_async_copy(turned, turned_out, sems.at[0])
    turned_copy.start()
    lag = (rows((length, length)) - lanes((length, length))).astype(f32)
    away = jnp.abs(lag)
    for h in range(4):
        g, i = h // 2, h % 2
        f, b = ld[0, g, i], ld[1, g, i]
        kr = keys[0] if g == 0 else keys[1 + i]
        weight = jnp.where(lag == 0, 2.0, jnp.exp(jnp.where(lag > 0, f, b) * away))
        a = (nt(of_head(queries, h), kr) * weight).astype(bf16)
        v = (v0 if g == 0 else v1)[:, i * 128 : (i + 1) * 128]
        inside[:, h * 128 : (h + 1) * 128] = nn(a, v)
    inside_copy = pltpu.make_async_copy(inside, inside_out, sems.at[1])
    inside_copy.start()
    turned_copy.wait()
    inside_copy.wait()


def finish_kernel(ld, turned_in, inside_in, enter_in, g0, g1, out, turned, inside, enter, sems):
    copies = [
        pltpu.make_async_copy(turned_in, turned, sems.at[0]),
        pltpu.make_async_copy(inside_in, inside, sems.at[1]),
    ]
    for copy in copies:
        copy.start()
    enter[...] = enter_in[...].astype(f32)
    length = turned.shape[0]
    t = rows((length, 128)).astype(f32)
    states = []
    for h in range(4):
        g, i = h // 2, h % 2
        if g == 0:
            e = [jnp.concatenate([enter[:, d, i, :]] * 2, 0) for d in range(2)]
        else:
            e = [jnp.concatenate([enter[:, d, 2 + 2 * i, :], enter[:, d, 3 + 2 * i, :]], 0) for d in range(2)]
        states.append(split(jnp.concatenate(e, 1)))
    for copy in copies:
        copy.wait()
    queries = [turned[:, k * 128 : (k + 1) * 128] for k in range(3)]
    for h in range(4):
        g, i = h // 2, h % 2
        f, b = ld[0, g, i], ld[1, g, i]
        q = of_head(queries, h)
        high, low = states[h]
        carried = nn(q, high) + nn(q, low)
        ret = (
            inside[:, h * 128 : (h + 1) * 128]
            + carried[:, :128] * jnp.exp(f * (t + 1.0))
            + carried[:, 128:] * jnp.exp(b * (length - t))
        )
        mean = jnp.mean(ret, -1, keepdims=True)
        centred = ret - mean
        variance = jnp.mean(centred * centred, -1, keepdims=True)
        gate = (g0 if g == 0 else g1)[:, i * 128 : (i + 1) * 128].astype(f32)
        y = gate * jax.nn.sigmoid(gate) * (centred * lax.rsqrt(variance + NORM_EPSILON))
        out[:, h * 128 : (h + 1) * 128] = y.astype(bf16)


def scan_kernel(ld, x, out):
    r = rows((8, 128))

    def factor(d):
        rate = jnp.full((8, 128), ld[d, 1, 1], f32)
        rate = jnp.where(r < 4, ld[d, 1, 0], rate)
        rate = jnp.where(r == 1, ld[d, 0, 1], rate)
        rate = jnp.where(r == 0, ld[d, 0, 0], rate)
        return jnp.exp(rate * 384.0)

    n = x.shape[0]
    forward, backward = factor(0), factor(1)
    acc = jnp.zeros((8, 128), f32)
    for k in range(n):
        out[k, 0] = acc.astype(STATE)
        acc = acc * forward + x[k, 0].astype(f32)
    acc = jnp.zeros((8, 128), f32)
    for k in reversed(range(n)):
        out[k, 1] = acc.astype(STATE)
        acc = acc * backward + x[k, 1].astype(f32)


def proj_kernel(place, y, stream, gain, own, *refs):
    others, (middle, normed, blocks, sems) = refs[:6], refs[6:]
    sources = [own.at[0], own.at[1], *others]
    copies = [pltpu.make_async_copy(s, blocks.at[k], sems.at[k]) for k, s in enumerate(sources)]
    for copy in copies:
        copy.start()
    tp, core = place[0], place[1]
    total = stream[...].astype(f32)
    for k, copy in enumerate(copies):
        if k < 2:
            rows_in = y[tp, :, k * 256 : (k + 1) * 256]
        else:
            piece = y[(tp + 4 - (k // 2)) % 4]
            first, _ = (core, 1 - core) if k % 2 == 0 else (1 - core, core)
            rows_in = jnp.where(first == 0, piece[:, :256], piece[:, 256:])
        copy.wait()
        part = nn(rows_in, blocks[k])
        proj = part if k == 0 else proj + part
    mid = (total + proj).astype(bf16)
    middle[...] = mid
    wide = mid.astype(f32)
    scale = lax.rsqrt(jnp.mean(wide * wide, -1, keepdims=True) + NORM_EPSILON)
    normed[...] = (wide * scale * gain[...]).astype(bf16)


SM = pl.BlockSpec(memory_space=pltpu.SMEM)
VM = pl.BlockSpec(memory_space=pltpu.VMEM)
HB = pl.BlockSpec(memory_space=pltpu.HBM)


def call(kernel, in_specs, outs, scratch=(), out_specs=None):
    return pl.pallas_call(
        kernel,
        in_specs=in_specs,
        out_specs=out_specs or jax.tree.map(lambda _: VM, outs),
        out_shape=outs,
        scratch_shapes=scratch,
        compiler_params=pltpu.CompilerParams(vmem_limit_bytes=40 * 2**20),
    )


def shape(*s, dtype=f32):
    return jax.ShapeDtypeStruct(s, dtype)


def exchanged(x, axis):
    return lax.all_to_all(x, axis, 0, 0, tiled=True)


def mixer_kernel(first, second, weights, out_a, out_b, held, act, hidden, sems):
    n, width = first.shape
    units = hidden.shape[1]
    step = width // STAGES
    spans = [pl.ds(k * step, step) for k in range(STAGES)]
    parts = [(span, pl.ds(at, size)) for at, size in ((0, 2 * units), (2 * units, units)) for span in spans]
    copies = [pltpu.make_async_copy(weights.at[p], held.at[p], sems.at[k]) for k, p in enumerate(parts)]
    for copy in copies:
        copy.start()
    for k, span in enumerate(spans):
        x = jnp.concatenate([first[:, span], second[:, span]], 0)
        copies[k].wait()
        part = nn(x, held[span, : 2 * units])
        act[...] = part if k == 0 else act[...] + part
    gate = act[:, :units]
    hidden[...] = (gate * jax.nn.sigmoid(gate) * act[:, units:]).astype(bf16)
    h = hidden[...]
    for k, span in enumerate(spans):
        copies[STAGES + k].wait()
        part = nt(h, held[span, 2 * units :]).astype(bf16)
        out_a[:, span] = part[:n]
        out_b[:, span] = part[n:]


def after(x, token):
    return lax.optimization_barrier((x, token))[0]


def in_hbm(x):
    return pltpu.with_memory_space_constraint(x, pltpu.HBM)


def shifted(x, by):
    n = lax.axis_size("tp")
    return lax.ppermute(x, "tp", [(k, (k + by) % n) for k in range(n)])


def body(
    stream,
    query_narrow,
    key_narrow,
    query_wide,
    key_wide,
    values,
    out_gate,
    out_weight,
    norm_gain,
    mlp_gate,
    mlp_up,
    mlp_down,
    log_decay,
):
    length, width = query_narrow.shape[0], stream.shape[1]
    hidden_units = mlp_gate.shape[1]
    shards = lax.all_gather(jnp.concatenate([mlp_gate, mlp_up, mlp_down.T], 1), SP, axis=0, tiled=True)

    rates = log_decay
    cosine, sine = angle_tables(length, lax.axis_index(SP) * length)
    v0, v1 = values[:, 0], values[:, 1]
    g0, g1 = out_gate[:, 0], out_gate[:, 1]
    states = shape(64, 2, 8, 128, dtype=STATE)
    state = call(state_kernel, [SM] + [VM] * 6, states, (pltpu.VMEM((64, 2, 8, 128), f32),))(
        rates, key_narrow, key_wide, v0, v1, cosine, sine
    )
    core = lax.axis_index("sp_2")
    half = lax.dynamic_index_in_dim(after(out_weight, state), core, 0, keepdims=False)
    same = []
    for s in (1, 2, 3):
        same.append(shifted(half, s))
    kept = [((length, 384), bf16), ((length, 512), f32)]
    turned, inside = call(
        inside_kernel,
        [SM] + [VM] * 8,
        tuple(pltpu.HBM(*k) for k in kept),
        tuple(pltpu.VMEM(*k) for k in kept) + (pltpu.SemaphoreType.DMA((2,)),),
        (HB, HB),
    )(rates, query_narrow, query_wide, key_narrow, key_wide, v0, v1, cosine, sine)
    arrived = exchanged(state, SP)
    enter = call(scan_kernel, [SM, VM], states)(rates, arrived)
    enter = exchanged(enter, SP)
    y = call(
        finish_kernel,
        [SM, HB, HB, VM, VM, VM],
        shape(length, 512, dtype=bf16),
        (pltpu.VMEM((length, 384), bf16), pltpu.VMEM((length, 512), f32), pltpu.VMEM((64, 2, 8, 128), f32), pltpu.SemaphoreType.DMA((2,))),
    )(rates, in_hbm(turned), in_hbm(inside), enter, g0, g1)
    other = []
    for s in (1, 2, 3):
        other.append(lax.ppermute(after(same[s - 1], y), "sp_2", [(0, 1), (1, 0)]))
    n_tp = lax.axis_size("tp")
    y = exchanged(y.reshape(n_tp, length // n_tp, 512), "tp")
    own = shape(length // n_tp, width, dtype=bf16)
    place = jnp.stack([lax.axis_index("tp"), core]).astype(jnp.int32)
    pieces = [w for pair in zip(same, other) for w in pair]
    middle, normed = call(
        proj_kernel,
        [SM, VM, VM, VM] + [HB] * 7,
        (own, own),
        (pltpu.VMEM((8, 256, width), bf16), pltpu.SemaphoreType.DMA((8,))),
    )(place, y, stream, norm_gain[None], in_hbm(out_weight), *pieces)

    def mixed(first, second):
        n, _ = first.shape
        return call(
            mixer_kernel,
            [VM, VM, HB],
            (own, own),
            (
                pltpu.VMEM(shards.shape, bf16),
                pltpu.VMEM((2 * n, 2 * hidden_units), f32),
                pltpu.VMEM((2 * n, hidden_units), bf16),
                pltpu.SemaphoreType.DMA((2 * STAGES,)),
            ),
        )(first, second, in_hbm(shards))

    to_third, to_first = mixed(shifted(normed, 1), shifted(normed, 3))
    arrivals = [shifted(to_third, 3), shifted(to_first, 1)]
    total, to_second = mixed(after(normed, to_first), shifted(normed, 2))
    arrivals.append(shifted(to_second, 2))
    total = total.astype(f32)
    for arrival in arrivals:
        total = total + arrival.astype(f32)
    return (middle.astype(f32) + 0.5 * total).astype(bf16)


def solution(mesh):
    finer = Mesh(mesh.devices.reshape(8, 4, 2, mesh.shape["tp"]), ("sp_0", "sp_1", "sp_2", "tp"))
    return jax.shard_map(
        body,
        mesh=finer,
        in_specs=(
            P(SP_TP, None),
            P(SP, "tp"),
            P(SP, "tp"),
            P(SP, "tp"),
            P(SP, "tp"),
            P(SP, None, "tp"),
            P(SP, None, "tp"),
            P(None, "tp", None),
            P(),
            P(SP, "tp"),
            P(SP, "tp"),
            P("tp", SP),
            P(None, None, "tp"),
        ),
        out_specs=P(SP_TP, None),
        check_vma=False,
    )
```

```python
import jax
import jax.numpy as jnp
from jax import lax
from jax.experimental import pallas as pl
from jax.experimental.pallas import tpu as pltpu
from jax.sharding import Mesh
from jax.sharding import PartitionSpec as P


SP = ("sp_0", "sp_1", "sp_2")
SP_TP = ("sp_0", "sp_1", "sp_2", "tp")

NORM_EPSILON = 1e-06
ROPE_BASE = 10000.0
f32, bf16 = jnp.float32, jnp.bfloat16


def angle_tables(length, first):
    positions = (first + jnp.arange(length, dtype=jnp.int32)).astype(f32)
    wide = jnp.power(ROPE_BASE, -(jnp.arange(64, dtype=f32) / 64))
    narrow = jnp.power(ROPE_BASE, -(jnp.arange(32, dtype=f32) / 32))
    angles = positions[:, None] * jnp.concatenate([wide, narrow, narrow])[None]
    return jnp.cos(angles), jnp.sin(angles)


def lanes(shape):
    return lax.broadcasted_iota(jnp.int32, shape, len(shape) - 1)


def rows(shape):
    return lax.broadcasted_iota(jnp.int32, shape, 0)


def turned_wide(u, cosine, sine):
    lane = lanes(u.shape)
    c = jnp.where(lane < 64, cosine, pltpu.roll(cosine, 64, 1))
    s = jnp.where(lane < 64, -sine, pltpu.roll(sine, 64, 1))
    return u * c + pltpu.roll(u, 64, 1) * s


def turned_narrow(u, cosine, sine):
    lane = lanes(u.shape)
    c = jnp.where(lane < 64, pltpu.roll(cosine, 64, 1), cosine)
    s = jnp.where(lane < 64, pltpu.roll(sine, 64, 1), sine)
    low = (lane & 32) == 0
    other = jnp.where(low, pltpu.roll(u, 96, 1), pltpu.roll(u, 32, 1))
    return u * c + other * jnp.where(low, -s, s)


def split(x):
    high = x.astype(bf16)
    return high, (x - high.astype(f32)).astype(bf16)


def nt(a, b):
    return lax.dot_general(a, b, (((1,), (1,)), ((), ())), preferred_element_type=f32)


def tn(a, b):
    return lax.dot_general(a, b, (((0,), (0,)), ((), ())), preferred_element_type=f32)


def nn(a, b):
    return jnp.dot(a, b, preferred_element_type=f32)


STATE = bf16
STAGES = 4


def turned_all(narrow, wide, cosine, sine, scales):
    c, s = cosine[...], sine[...]
    parts = [turned_narrow(narrow[...].astype(f32), c, s) * scales[0]]
    for i in range(2):
        parts.append(turned_wide(wide[:, i * 128 : (i + 1) * 128].astype(f32), c, s) * scales[1])
    return [p.astype(bf16) for p in parts]


def of_head(parts, h):
    if h >= 2:
        return parts[h - 1]
    return jnp.where((lanes(parts[0].shape) // 64) == h, parts[0], jnp.zeros_like(parts[0]))


KEY_SCALES = (64**-0.5, 128**-0.5)


def state_kernel(ld, kn, kw, v0, v1, cosine, sine, out, state):
    length = kn.shape[0]
    keys = turned_all(kn, kw, cosine, sine, KEY_SCALES)
    t = rows((length, 128)).astype(f32)
    for h in range(4):
        g, i = h // 2, h % 2
        f, b = ld[0, g, i], ld[1, g, i]
        v = (v0 if g == 0 else v1)[:, i * 128 : (i + 1) * 128].astype(f32)
        scaled = jnp.concatenate([v * jnp.exp(f * (length - 1.0 - t)), v * jnp.exp(b * t)], 1)
        high, low = split(scaled)
        kr = keys[0] if g == 0 else keys[1 + i]
        total = tn(kr, high) + tn(kr, low)
        for d in range(2):
            part = total[:, d * 128 : (d + 1) * 128]
            if g == 0:
                state[:, d, i, :] = part[i * 64 : (i + 1) * 64]
            else:
                state[:, d, 2 + 2 * i, :] = part[:64]
                state[:, d, 3 + 2 * i, :] = part[64:]
    for d in range(2):
        for r in (6, 7):
            state[:, d, r, :] = jnp.zeros((64, 128), f32)
    out[...] = state[...].astype(STATE)


def inside_kernel(ld, qn, qw, kn, kw, v0, v1, cosine, sine, turned_out, inside_out, turned, inside, sems):
    length = qn.shape[0]
    queries = turned_all(qn, qw, cosine, sine, (1.0, 1.0))
    keys = turned_all(kn, kw, cosine, sine, KEY_SCALES)
    for k in range(3):
        turned[:, k * 128 : (k + 1) * 128] = queries[k]
    turned_copy = pltpu.make_async_copy(turned, turned_out, sems.at[0])
    turned_copy.start()
    lag = (rows((length, length)) - lanes((length, length))).astype(f32)
    away = jnp.abs(lag)
    for h in range(4):
        g, i = h // 2, h % 2
        f, b = ld[0, g, i], ld[1, g, i]
        kr = keys[0] if g == 0 else keys[1 + i]
        weight = jnp.where(lag == 0, 2.0, jnp.exp(jnp.where(lag > 0, f, b) * away))
        a = (nt(of_head(queries, h), kr) * weight).astype(bf16)
        v = (v0 if g == 0 else v1)[:, i * 128 : (i + 1) * 128]
        inside[:, h * 128 : (h + 1) * 128] = nn(a, v)
    inside_copy = pltpu.make_async_copy(inside, inside_out, sems.at[1])
    inside_copy.start()
    turned_copy.wait()
    inside_copy.wait()


def finish_kernel(ld, turned_in, inside_in, enter_in, g0, g1, out, turned, inside, enter, sems):
    copies = [
        pltpu.make_async_copy(turned_in, turned, sems.at[0]),
        pltpu.make_async_copy(inside_in, inside, sems.at[1]),
    ]
    for copy in copies:
        copy.start()
    enter[...] = enter_in[...].astype(f32)
    length = turned.shape[0]
    t = rows((length, 128)).astype(f32)
    states = []
    for h in range(4):
        g, i = h // 2, h % 2
        if g == 0:
            e = [jnp.concatenate([enter[:, d, i, :]] * 2, 0) for d in range(2)]
        else:
            e = [jnp.concatenate([enter[:, d, 2 + 2 * i, :], enter[:, d, 3 + 2 * i, :]], 0) for d in range(2)]
        states.append(split(jnp.concatenate(e, 1)))
    for copy in copies:
        copy.wait()
    queries = [turned[:, k * 128 : (k + 1) * 128] for k in range(3)]
    for h in range(4):
        g, i = h // 2, h % 2
        f, b = ld[0, g, i], ld[1, g, i]
        q = of_head(queries, h)
        high, low = states[h]
        carried = nn(q, high) + nn(q, low)
        ret = (
            inside[:, h * 128 : (h + 1) * 128]
            + carried[:, :128] * jnp.exp(f * (t + 1.0))
            + carried[:, 128:] * jnp.exp(b * (length - t))
        )
        mean = jnp.mean(ret, -1, keepdims=True)
        centred = ret - mean
        variance = jnp.mean(centred * centred, -1, keepdims=True)
        gate = (g0 if g == 0 else g1)[:, i * 128 : (i + 1) * 128].astype(f32)
        y = gate * jax.nn.sigmoid(gate) * (centred * lax.rsqrt(variance + NORM_EPSILON))
        out[:, h * 128 : (h + 1) * 128] = y.astype(bf16)


def scan_kernel(ld, x, out):
    r = rows((8, 128))

    def factor(d):
        rate = jnp.full((8, 128), ld[d, 1, 1], f32)
        rate = jnp.where(r < 4, ld[d, 1, 0], rate)
        rate = jnp.where(r == 1, ld[d, 0, 1], rate)
        rate = jnp.where(r == 0, ld[d, 0, 0], rate)
        return jnp.exp(rate * 384.0)

    n = x.shape[0]
    forward, backward = factor(0), factor(1)
    acc = jnp.zeros((8, 128), f32)
    for k in range(n):
        out[k, 0] = acc.astype(STATE)
        acc = acc * forward + x[k, 0].astype(f32)
    acc = jnp.zeros((8, 128), f32)
    for k in reversed(range(n)):
        out[k, 1] = acc.astype(STATE)
        acc = acc * backward + x[k, 1].astype(f32)


def proj_kernel(place, y, stream, gain, own, *refs):
    others, (middle, normed, blocks, sems) = refs[:6], refs[6:]
    sources = [own.at[0], own.at[1], *others]
    copies = [pltpu.make_async_copy(s, blocks.at[k], sems.at[k]) for k, s in enumerate(sources)]
    for copy in copies:
        copy.start()
    tp, core = place[0], place[1]
    total = stream[...].astype(f32)
    for k, copy in enumerate(copies):
        if k < 2:
            rows_in = y[tp, :, k * 256 : (k + 1) * 256]
        else:
            piece = y[(tp + 4 - (k // 2)) % 4]
            first, _ = (core, 1 - core) if k % 2 == 0 else (1 - core, core)
            rows_in = jnp.where(first == 0, piece[:, :256], piece[:, 256:])
        copy.wait()
        part = nn(rows_in, blocks[k])
        proj = part if k == 0 else proj + part
    mid = (total + proj).astype(bf16)
    middle[...] = mid
    wide = mid.astype(f32)
    scale = lax.rsqrt(jnp.mean(wide * wide, -1, keepdims=True) + NORM_EPSILON)
    normed[...] = (wide * scale * gain[...]).astype(bf16)


SM = pl.BlockSpec(memory_space=pltpu.SMEM)
VM = pl.BlockSpec(memory_space=pltpu.VMEM)
HB = pl.BlockSpec(memory_space=pltpu.HBM)


def call(kernel, in_specs, outs, scratch=(), out_specs=None, room=40):
    return pl.pallas_call(
        kernel,
        in_specs=in_specs,
        out_specs=out_specs or jax.tree.map(lambda _: VM, outs),
        out_shape=outs,
        scratch_shapes=scratch,
        compiler_params=pltpu.CompilerParams(vmem_limit_bytes=room * 2**20),
    )


def shape(*s, dtype=f32):
    return jax.ShapeDtypeStruct(s, dtype)


def exchanged(x, axis):
    return lax.all_to_all(x, axis, 0, 0, tiled=True)


def weight_parts(width, units):
    step = width // STAGES
    spans = [pl.ds(k * step, step) for k in range(STAGES)]
    return spans, [(span, pl.ds(at, size)) for at, size in ((0, 2 * units), (2 * units, units)) for span in spans]


def mixed_into(pieces, held, outs, act, hidden, ready):
    n = pieces[0].shape[0]
    units = hidden.shape[1]
    spans, _ = weight_parts(held.shape[0], units)
    for k, span in enumerate(spans):
        x = jnp.concatenate([p[:, span] for p in pieces], 0)
        ready(k)
        part = nn(x, held[span, : 2 * units])
        act[...] = part if k == 0 else act[...] + part
    gate = act[:, :units]
    hidden[...] = (gate * jax.nn.sigmoid(gate) * act[:, units:]).astype(bf16)
    h = hidden[...]
    for k, span in enumerate(spans):
        ready(STAGES + k)
        part = nt(h, held[span, 2 * units :]).astype(bf16)
        for j, out in enumerate(outs):
            out[:, span] = part[j * n : (j + 1) * n]


def first_mixer(piece, weights, out, held, act, hidden, sems):
    _, parts = weight_parts(held.shape[0], hidden.shape[1])
    copies = [pltpu.make_async_copy(weights.at[p], held.at[p], sems.at[k]) for k, p in enumerate(parts)]
    for copy in copies:
        copy.start()
    mixed_into([piece], held, [out], act, hidden, lambda k: copies[k].wait())


def near_mixer(first, second, held, out_a, out_b, act, hidden):
    mixed_into([first, second], held, [out_a, out_b], act, hidden, lambda k: None)


def own_mixer(piece, held, out, act, hidden):
    mixed_into([piece], held, [out], act, hidden, lambda k: None)


def after(x, token):
    return lax.optimization_barrier((x, token))[0]


def in_hbm(x):
    return pltpu.with_memory_space_constraint(x, pltpu.HBM)


def in_vmem(x):
    return pltpu.with_memory_space_constraint(x, pltpu.VMEM)


def shifted(x, by):
    n = lax.axis_size("tp")
    return lax.ppermute(x, "tp", [(k, (k + by) % n) for k in range(n)])


def body(
    stream,
    query_narrow,
    key_narrow,
    query_wide,
    key_wide,
    values,
    out_gate,
    out_weight,
    norm_gain,
    mlp_gate,
    mlp_up,
    mlp_down,
    log_decay,
):
    length, width = query_narrow.shape[0], stream.shape[1]
    hidden_units = mlp_gate.shape[1]
    shards = lax.all_gather(jnp.concatenate([mlp_gate, mlp_up, mlp_down.T], 1), SP, axis=0, tiled=True)

    rates = in_hbm(log_decay)
    query_narrow, query_wide, key_narrow, key_wide = map(in_hbm, (query_narrow, query_wide, key_narrow, key_wide))
    cosine, sine = angle_tables(length, lax.axis_index(SP) * length)
    v0, v1 = values[:, 0], values[:, 1]
    g0, g1 = out_gate[:, 0], out_gate[:, 1]
    states = shape(64, 2, 8, 128, dtype=STATE)
    state = call(state_kernel, [SM] + [VM] * 6, states, (pltpu.VMEM((64, 2, 8, 128), f32),))(
        rates, key_narrow, key_wide, v0, v1, cosine, sine
    )
    core = lax.axis_index("sp_2")
    half = lax.dynamic_index_in_dim(after(out_weight, state), core, 0, keepdims=False)
    same = []
    for s in (1, 2, 3):
        same.append(shifted(half, s))
    kept = [((length, 384), bf16), ((length, 512), f32)]
    turned, inside = call(
        inside_kernel,
        [SM] + [VM] * 8,
        tuple(pltpu.HBM(*k) for k in kept),
        tuple(pltpu.VMEM(*k) for k in kept) + (pltpu.SemaphoreType.DMA((2,)),),
        (HB, HB),
    )(rates, query_narrow, query_wide, key_narrow, key_wide, v0, v1, cosine, sine)
    arrived = exchanged(state, SP)
    enter = call(scan_kernel, [SM, VM], states)(rates, arrived)
    enter = exchanged(enter, SP)
    y = call(
        finish_kernel,
        [SM, HB, HB, VM, VM, VM],
        shape(length, 512, dtype=bf16),
        (pltpu.VMEM((length, 384), bf16), pltpu.VMEM((length, 512), f32), pltpu.VMEM((64, 2, 8, 128), f32), pltpu.SemaphoreType.DMA((2,))),
    )(rates, in_hbm(turned), in_hbm(inside), enter, g0, g1)
    other = []
    for s in (1, 2, 3):
        other.append(lax.ppermute(after(same[s - 1], y), "sp_2", [(0, 1), (1, 0)]))
    n_tp = lax.axis_size("tp")
    y = exchanged(y.reshape(n_tp, length // n_tp, 512), "tp")
    own = shape(length // n_tp, width, dtype=bf16)
    place = jnp.stack([lax.axis_index("tp"), core]).astype(jnp.int32)
    pieces = [w for pair in zip(same, other) for w in pair]
    middle, normed = call(
        proj_kernel,
        [SM, VM, VM, VM] + [HB] * 7,
        (own, own),
        (pltpu.VMEM((8, 256, width), bf16), pltpu.SemaphoreType.DMA((8,))),
    )(place, y, in_hbm(stream), in_hbm(norm_gain[None]), in_hbm(out_weight), *pieces)

    def room(pieces):
        m = pieces * own.shape[0]
        return (pltpu.VMEM((m, 2 * hidden_units), f32), pltpu.VMEM((m, hidden_units), bf16))

    around = [None] + [shifted(normed, s) for s in (1, 2, 3)]
    to_second, held = call(
        first_mixer,
        [VM, HB],
        (own, pltpu.VMEM(shards.shape, bf16)),
        room(1) + (pltpu.SemaphoreType.DMA((2 * STAGES,)),),
        room=12,
    )(around[2], in_hbm(shards))
    arrivals = [shifted(to_second, 2)]
    to_third, to_first = call(near_mixer, [VM] * 3, (own, own), room(2), room=12)(around[1], around[3], in_vmem(held))
    arrivals.append(shifted(to_third, 3))
    arrivals.append(shifted(to_first, 1))
    total = call(own_mixer, [VM] * 2, own, room(1), room=12)(after(normed, to_first), in_vmem(held))
    total = total.astype(f32)
    for arrival in arrivals:
        total = total + arrival.astype(f32)
    return (middle.astype(f32) + 0.5 * total).astype(bf16)


def solution(mesh):
    finer = Mesh(mesh.devices.reshape(8, 4, 2, mesh.shape["tp"]), ("sp_0", "sp_1", "sp_2", "tp"))
    return jax.shard_map(
        body,
        mesh=finer,
        in_specs=(
            P(SP_TP, None),
            P(SP, "tp"),
            P(SP, "tp"),
            P(SP, "tp"),
            P(SP, "tp"),
            P(SP, None, "tp"),
            P(SP, None, "tp"),
            P(None, "tp", None),
            P(),
            P(SP, "tp"),
            P(SP, "tp"),
            P("tp", SP),
            P(None, None, "tp"),
        ),
        out_specs=P(SP_TP, None),
        check_vma=False,
    )
```

```python
import jax
import jax.numpy as jnp
from jax import lax
from jax.experimental import pallas as pl
from jax.experimental.pallas import tpu as pltpu
from jax.sharding import Mesh
from jax.sharding import PartitionSpec as P


SP = ("sp_0", "sp_1", "sp_2")
SP_TP = ("sp_0", "sp_1", "sp_2", "tp")

NORM_EPSILON = 1e-06
ROPE_BASE = 10000.0
f32, bf16 = jnp.float32, jnp.bfloat16


def angle_tables(length, first):
    positions = (first + jnp.arange(length, dtype=jnp.int32)).astype(f32)
    wide = jnp.power(ROPE_BASE, -(jnp.arange(64, dtype=f32) / 64))
    narrow = jnp.power(ROPE_BASE, -(jnp.arange(32, dtype=f32) / 32))
    angles = positions[:, None] * jnp.concatenate([wide, narrow, narrow])[None]
    return jnp.cos(angles), jnp.sin(angles)


def lanes(shape):
    return lax.broadcasted_iota(jnp.int32, shape, len(shape) - 1)


def rows(shape):
    return lax.broadcasted_iota(jnp.int32, shape, 0)


def turned_wide(u, cosine, sine):
    lane = lanes(u.shape)
    c = jnp.where(lane < 64, cosine, pltpu.roll(cosine, 64, 1))
    s = jnp.where(lane < 64, -sine, pltpu.roll(sine, 64, 1))
    return u * c + pltpu.roll(u, 64, 1) * s


def turned_narrow(u, cosine, sine):
    lane = lanes(u.shape)
    c = jnp.where(lane < 64, pltpu.roll(cosine, 64, 1), cosine)
    s = jnp.where(lane < 64, pltpu.roll(sine, 64, 1), sine)
    low = (lane & 32) == 0
    other = jnp.where(low, pltpu.roll(u, 96, 1), pltpu.roll(u, 32, 1))
    return u * c + other * jnp.where(low, -s, s)


def split(x):
    high = x.astype(bf16)
    return high, (x - high.astype(f32)).astype(bf16)


def nt(a, b):
    return lax.dot_general(a, b, (((1,), (1,)), ((), ())), preferred_element_type=f32)


def tn(a, b):
    return lax.dot_general(a, b, (((0,), (0,)), ((), ())), preferred_element_type=f32)


def nn(a, b):
    return jnp.dot(a, b, preferred_element_type=f32)


STATE = bf16
STAGES = 4
STEPS = (0, 1, -1, 2, -2, 3, -3, 4)


def turned_all(narrow, wide, cosine, sine, scales):
    c, s = cosine[...], sine[...]
    parts = [turned_narrow(narrow[...].astype(f32), c, s) * scales[0]]
    for i in range(2):
        parts.append(turned_wide(wide[:, i * 128 : (i + 1) * 128].astype(f32), c, s) * scales[1])
    return [p.astype(bf16) for p in parts]


def of_head(parts, h):
    if h >= 2:
        return parts[h - 1]
    return jnp.where((lanes(parts[0].shape) // 64) == h, parts[0], jnp.zeros_like(parts[0]))


KEY_SCALES = (64**-0.5, 128**-0.5)


def state_kernel(ld, kn, kw, v0, v1, cosine, sine, out, state):
    length = kn.shape[0]
    keys = turned_all(kn, kw, cosine, sine, KEY_SCALES)
    t = rows((length, 128)).astype(f32)
    for h in range(4):
        g, i = h // 2, h % 2
        f, b = ld[0, g, i], ld[1, g, i]
        v = (v0 if g == 0 else v1)[:, i * 128 : (i + 1) * 128].astype(f32)
        scaled = jnp.concatenate([v * jnp.exp(f * (length - 1.0 - t)), v * jnp.exp(b * t)], 1)
        high, low = split(scaled)
        kr = keys[0] if g == 0 else keys[1 + i]
        total = tn(kr, high) + tn(kr, low)
        for d in range(2):
            part = total[:, d * 128 : (d + 1) * 128]
            if g == 0:
                state[:, d, i, :] = part[i * 64 : (i + 1) * 64]
            else:
                state[:, d, 2 + 2 * i, :] = part[:64]
                state[:, d, 3 + 2 * i, :] = part[64:]
    for d in range(2):
        for r in (6, 7):
            state[:, d, r, :] = jnp.zeros((64, 128), f32)
    out[...] = state[...].astype(STATE)


def inside_kernel(ld, qn, qw, kn, kw, v0, v1, cosine, sine, turned_out, inside_out, turned, inside, sems):
    length = qn.shape[0]
    queries = turned_all(qn, qw, cosine, sine, (1.0, 1.0))
    keys = turned_all(kn, kw, cosine, sine, KEY_SCALES)
    for k in range(3):
        turned[:, k * 128 : (k + 1) * 128] = queries[k]
    turned_copy = pltpu.make_async_copy(turned, turned_out, sems.at[0])
    turned_copy.start()
    lag = (rows((length, length)) - lanes((length, length))).astype(f32)
    away = jnp.abs(lag)
    for h in range(4):
        g, i = h // 2, h % 2
        f, b = ld[0, g, i], ld[1, g, i]
        kr = keys[0] if g == 0 else keys[1 + i]
        weight = jnp.where(lag == 0, 2.0, jnp.exp(jnp.where(lag > 0, f, b) * away))
        a = (nt(of_head(queries, h), kr) * weight).astype(bf16)
        v = (v0 if g == 0 else v1)[:, i * 128 : (i + 1) * 128]
        inside[:, h * 128 : (h + 1) * 128] = nn(a, v)
    inside_copy = pltpu.make_async_copy(inside, inside_out, sems.at[1])
    inside_copy.start()
    turned_copy.wait()
    inside_copy.wait()


def finish_kernel(ld, turned_in, inside_in, enter_in, g0, g1, out, turned, inside, enter, sems):
    copies = [
        pltpu.make_async_copy(turned_in, turned, sems.at[0]),
        pltpu.make_async_copy(inside_in, inside, sems.at[1]),
    ]
    for copy in copies:
        copy.start()
    enter[...] = enter_in[...].astype(f32)
    length = turned.shape[0]
    t = rows((length, 128)).astype(f32)
    states = []
    for h in range(4):
        g, i = h // 2, h % 2
        if g == 0:
            e = [jnp.concatenate([enter[:, d, i, :]] * 2, 0) for d in range(2)]
        else:
            e = [jnp.concatenate([enter[:, d, 2 + 2 * i, :], enter[:, d, 3 + 2 * i, :]], 0) for d in range(2)]
        states.append(split(jnp.concatenate(e, 1)))
    for copy in copies:
        copy.wait()
    queries = [turned[:, k * 128 : (k + 1) * 128] for k in range(3)]
    for h in range(4):
        g, i = h // 2, h % 2
        f, b = ld[0, g, i], ld[1, g, i]
        q = of_head(queries, h)
        high, low = states[h]
        carried = nn(q, high) + nn(q, low)
        ret = (
            inside[:, h * 128 : (h + 1) * 128]
            + carried[:, :128] * jnp.exp(f * (t + 1.0))
            + carried[:, 128:] * jnp.exp(b * (length - t))
        )
        mean = jnp.mean(ret, -1, keepdims=True)
        centred = ret - mean
        variance = jnp.mean(centred * centred, -1, keepdims=True)
        gate = (g0 if g == 0 else g1)[:, i * 128 : (i + 1) * 128].astype(f32)
        y = gate * jax.nn.sigmoid(gate) * (centred * lax.rsqrt(variance + NORM_EPSILON))
        out[:, h * 128 : (h + 1) * 128] = y.astype(bf16)


def scan_kernel(ld, x, out):
    r = rows((8, 128))

    def factor(d):
        rate = jnp.full((8, 128), ld[d, 1, 1], f32)
        rate = jnp.where(r < 4, ld[d, 1, 0], rate)
        rate = jnp.where(r == 1, ld[d, 0, 1], rate)
        rate = jnp.where(r == 0, ld[d, 0, 0], rate)
        return jnp.exp(rate * 384.0)

    n = x.shape[0]
    forward, backward = factor(0), factor(1)
    acc = jnp.zeros((8, 128), f32)
    for k in range(n):
        out[k, 0] = acc.astype(STATE)
        acc = acc * forward + x[k, 0].astype(f32)
    acc = jnp.zeros((8, 128), f32)
    for k in reversed(range(n)):
        out[k, 1] = acc.astype(STATE)
        acc = acc * backward + x[k, 1].astype(f32)


def proj_kernel(place, y, stream, gain, own, *refs):
    others, (middle, normed, blocks, sems) = refs[:6], refs[6:]
    sources = [own.at[0], own.at[1], *others]
    copies = [pltpu.make_async_copy(s, blocks.at[k], sems.at[k]) for k, s in enumerate(sources)]
    for copy in copies:
        copy.start()
    tp, core = place[0], place[1]
    total = stream[...].astype(f32)
    for k, copy in enumerate(copies):
        if k < 2:
            rows_in = y[tp, :, k * 256 : (k + 1) * 256]
        else:
            piece = y[(tp + 4 - (k // 2)) % 4]
            first, _ = (core, 1 - core) if k % 2 == 0 else (1 - core, core)
            rows_in = jnp.where(first == 0, piece[:, :256], piece[:, 256:])
        copy.wait()
        part = nn(rows_in, blocks[k])
        proj = part if k == 0 else proj + part
    mid = (total + proj).astype(bf16)
    middle[...] = mid
    wide = mid.astype(f32)
    scale = lax.rsqrt(jnp.mean(wide * wide, -1, keepdims=True) + NORM_EPSILON)
    normed[...] = (wide * scale * gain[...]).astype(bf16)


SM = pl.BlockSpec(memory_space=pltpu.SMEM)
VM = pl.BlockSpec(memory_space=pltpu.VMEM)
HB = pl.BlockSpec(memory_space=pltpu.HBM)


def call(kernel, in_specs, outs, scratch=(), out_specs=None, room=40):
    return pl.pallas_call(
        kernel,
        in_specs=in_specs,
        out_specs=out_specs or jax.tree.map(lambda _: VM, outs),
        out_shape=outs,
        scratch_shapes=scratch,
        compiler_params=pltpu.CompilerParams(vmem_limit_bytes=room * 2**20),
    )


def shape(*s, dtype=f32):
    return jax.ShapeDtypeStruct(s, dtype)


def exchanged(x, axis):
    return lax.all_to_all(x, axis, 0, 0, tiled=True)


def mixed_into(pieces, rising, falling, outs, act, hidden, ready):
    n, width = pieces[0].shape
    units = hidden.shape[1]
    step = width // STAGES
    spans = [pl.ds(k * step, step) for k in range(STAGES)]
    for k, span in enumerate(spans):
        x = jnp.concatenate([p[:, span] for p in pieces], 0)
        ready(k)
        part = nn(x, rising[span, :])
        act[...] = part if k == 0 else act[...] + part
    gate = act[:, :units]
    hidden[...] = (gate * jax.nn.sigmoid(gate) * act[:, units:]).astype(bf16)
    h = hidden[...]
    ready(STAGES)
    for span in spans:
        part = nt(h, falling[span, :]).astype(bf16)
        for j, out in enumerate(outs):
            out[:, span] = part[j * n : (j + 1) * n]


def first_mixer(seat, piece, weights, *refs):
    blocks, (out, rising, falling, act, hidden, sems, block_sems) = refs[:16], refs[16:]
    z, x, core = seat[0], seat[1], seat[2]
    step = weights.shape[0] // STAGES
    copies = [
        pltpu.make_async_copy(weights.at[pl.ds(k * step, step)], rising.at[pl.ds(k * step, step)], sems.at[k])
        for k in range(STAGES)
    ]
    later = []
    for k, away in enumerate(STEPS):
        for c in range(2):
            owner = core if c == 0 else 1 - core
            for j in range(4):
                row = ((z + 8 - away) % 8) * 256 + ((x + 4 - j) % 4) * 64 + owner * 32
                target = falling.at[pl.ds(pl.multiple_of(row, 32), 32)]
                later.append(pltpu.make_async_copy(blocks[2 * k + c].at[j], target, block_sems.at[k, c, j]))
    for copy in copies + later:
        copy.start()

    def ready(k):
        for copy in [copies[k]] if k < STAGES else later:
            copy.wait()

    mixed_into([piece], rising, falling, [out], act, hidden, ready)


def near_mixer(first, second, rising, falling, out_a, out_b, act, hidden):
    mixed_into([first, second], rising, falling, [out_a, out_b], act, hidden, lambda k: None)


def own_mixer(piece, rising, falling, out, act, hidden):
    mixed_into([piece], rising, falling, [out], act, hidden, lambda k: None)


def relayed(x, axis, by):
    n = lax.axis_size(axis)
    return lax.ppermute(x, axis, [(k, (k + by) % n) for k in range(n)])


def after(x, token):
    return lax.optimization_barrier((x, token))[0]


def in_hbm(x):
    return pltpu.with_memory_space_constraint(x, pltpu.HBM)


def in_vmem(x):
    return pltpu.with_memory_space_constraint(x, pltpu.VMEM)


def shifted(x, by):
    n = lax.axis_size("tp")
    return lax.ppermute(x, "tp", [(k, (k + by) % n) for k in range(n)])


def body(
    stream,
    query_narrow,
    key_narrow,
    query_wide,
    key_wide,
    values,
    out_gate,
    out_weight,
    norm_gain,
    mlp_gate,
    mlp_up,
    mlp_down,
    log_decay,
):
    length, width = query_narrow.shape[0], stream.shape[1]
    hidden_units = mlp_gate.shape[1]
    shards = lax.all_gather(jnp.concatenate([mlp_gate, mlp_up], 1), SP, axis=0, tiled=True)

    rates = in_hbm(log_decay)
    query_narrow, query_wide, key_narrow, key_wide = map(in_hbm, (query_narrow, query_wide, key_narrow, key_wide))
    cosine, sine = angle_tables(length, lax.axis_index(SP) * length)
    v0, v1 = values[:, 0], values[:, 1]
    g0, g1 = out_gate[:, 0], out_gate[:, 1]
    states = shape(64, 2, 8, 128, dtype=STATE)
    state = call(state_kernel, [SM] + [VM] * 6, states, (pltpu.VMEM((64, 2, 8, 128), f32),))(
        rates, key_narrow, key_wide, v0, v1, cosine, sine
    )
    core = lax.axis_index("sp_2")
    mine = after(mlp_down.T, state)
    beside = [mine] + [relayed(mine, "sp_1", s) for s in (1, 2, 3)]
    block = jnp.stack(beside)
    held = {0: block}
    for step in (1, 2, 3, 4):
        held[step] = relayed(held[step - 1], "sp_0", 1)
        if step < 4:
            held[-step] = relayed(held[1 - step], "sp_0", -1)
    half = lax.dynamic_index_in_dim(after(out_weight, state), core, 0, keepdims=False)
    same = []
    for s in (1, 2, 3):
        same.append(shifted(half, s))
    kept = [((length, 384), bf16), ((length, 512), f32)]
    turned, inside = call(
        inside_kernel,
        [SM] + [VM] * 8,
        tuple(pltpu.HBM(*k) for k in kept),
        tuple(pltpu.VMEM(*k) for k in kept) + (pltpu.SemaphoreType.DMA((2,)),),
        (HB, HB),
    )(rates, query_narrow, query_wide, key_narrow, key_wide, v0, v1, cosine, sine)
    arrived = exchanged(state, SP)
    enter = call(scan_kernel, [SM, VM], states)(rates, arrived)
    enter = exchanged(enter, SP)
    y = call(
        finish_kernel,
        [SM, HB, HB, VM, VM, VM],
        shape(length, 512, dtype=bf16),
        (pltpu.VMEM((length, 384), bf16), pltpu.VMEM((length, 512), f32), pltpu.VMEM((64, 2, 8, 128), f32), pltpu.SemaphoreType.DMA((2,))),
    )(rates, in_hbm(turned), in_hbm(inside), enter, g0, g1)
    other = []
    for s in (1, 2, 3):
        other.append(lax.ppermute(after(same[s - 1], y), "sp_2", [(0, 1), (1, 0)]))
    n_tp = lax.axis_size("tp")
    y = exchanged(y.reshape(n_tp, length // n_tp, 512), "tp")
    own = shape(length // n_tp, width, dtype=bf16)
    place = jnp.stack([lax.axis_index("tp"), core]).astype(jnp.int32)
    pieces = [w for pair in zip(same, other) for w in pair]
    middle, normed = call(
        proj_kernel,
        [SM, VM, VM, VM] + [HB] * 7,
        (own, own),
        (pltpu.VMEM((8, 256, width), bf16), pltpu.SemaphoreType.DMA((8,))),
    )(place, y, in_hbm(stream), in_hbm(norm_gain[None]), in_hbm(out_weight), *pieces)

    def room(pieces):
        m = pieces * own.shape[0]
        return (pltpu.VMEM((m, 2 * hidden_units), f32), pltpu.VMEM((m, hidden_units), bf16))

    around = [None] + [relayed(normed, "tp", s) for s in (1, 2, 3)]
    pairs = []
    for step in STEPS:
        pairs += [held[step], relayed(held[step], "sp_2", 1)]
    seat = jnp.stack([lax.axis_index(axis) for axis in SP]).astype(jnp.int32)
    to_second, rising, falling = call(
        first_mixer,
        [SM, VM, HB] + [HB] * 16,
        (own, pltpu.VMEM(shards.shape, bf16), pltpu.VMEM((width, hidden_units), bf16)),
        room(1) + (pltpu.SemaphoreType.DMA((STAGES,)), pltpu.SemaphoreType.DMA((8, 2, 4))),
        room=12,
    )(seat, around[2], in_hbm(shards), *map(in_hbm, pairs))
    rising, falling = in_vmem(rising), in_vmem(falling)
    arrivals = [shifted(to_second, 2)]
    to_third, to_first = call(near_mixer, [VM] * 4, (own, own), room(2), room=12)(around[1], around[3], rising, falling)
    arrivals.append(shifted(to_third, 3))
    arrivals.append(shifted(to_first, 1))
    total = call(own_mixer, [VM] * 3, own, room(1), room=12)(after(normed, to_first), rising, falling)
    total = total.astype(f32)
    for arrival in arrivals:
        total = total + arrival.astype(f32)
    return (middle.astype(f32) + 0.5 * total).astype(bf16)


def solution(mesh):
    finer = Mesh(mesh.devices.reshape(8, 4, 2, mesh.shape["tp"]), ("sp_0", "sp_1", "sp_2", "tp"))
    return jax.shard_map(
        body,
        mesh=finer,
        in_specs=(
            P(SP_TP, None),
            P(SP, "tp"),
            P(SP, "tp"),
            P(SP, "tp"),
            P(SP, "tp"),
            P(SP, None, "tp"),
            P(SP, None, "tp"),
            P(None, "tp", None),
            P(),
            P(SP, "tp"),
            P(SP, "tp"),
            P("tp", SP),
            P(None, None, "tp"),
        ),
        out_specs=P(SP_TP, None),
        check_vma=False,
    )
```

```python
import jax
import jax.numpy as jnp
from jax import lax
from jax.experimental import pallas as pl
from jax.experimental.pallas import tpu as pltpu
from jax.sharding import Mesh
from jax.sharding import PartitionSpec as P


SP = ("sp_0", "sp_1", "sp_2")
SP_TP = ("sp_0", "sp_1", "sp_2", "tp")

NORM_EPSILON = 1e-06
ROPE_BASE = 10000.0
f32, bf16 = jnp.float32, jnp.bfloat16


def angle_tables(length, first):
    positions = (first + jnp.arange(length, dtype=jnp.int32)).astype(f32)
    wide = jnp.power(ROPE_BASE, -(jnp.arange(64, dtype=f32) / 64))
    narrow = jnp.power(ROPE_BASE, -(jnp.arange(32, dtype=f32) / 32))
    angles = positions[:, None] * jnp.concatenate([wide, narrow, narrow])[None]
    return jnp.cos(angles), jnp.sin(angles)


def lanes(shape):
    return lax.broadcasted_iota(jnp.int32, shape, len(shape) - 1)


def rows(shape):
    return lax.broadcasted_iota(jnp.int32, shape, 0)


def turned_wide(u, cosine, sine):
    lane = lanes(u.shape)
    c = jnp.where(lane < 64, cosine, pltpu.roll(cosine, 64, 1))
    s = jnp.where(lane < 64, -sine, pltpu.roll(sine, 64, 1))
    return u * c + pltpu.roll(u, 64, 1) * s


def turned_narrow(u, cosine, sine):
    lane = lanes(u.shape)
    c = jnp.where(lane < 64, pltpu.roll(cosine, 64, 1), cosine)
    s = jnp.where(lane < 64, pltpu.roll(sine, 64, 1), sine)
    low = (lane & 32) == 0
    other = jnp.where(low, pltpu.roll(u, 96, 1), pltpu.roll(u, 32, 1))
    return u * c + other * jnp.where(low, -s, s)


def split(x):
    high = x.astype(bf16)
    return high, (x - high.astype(f32)).astype(bf16)


def nt(a, b):
    return lax.dot_general(a, b, (((1,), (1,)), ((), ())), preferred_element_type=f32)


def tn(a, b):
    return lax.dot_general(a, b, (((0,), (0,)), ((), ())), preferred_element_type=f32)


def nn(a, b):
    return jnp.dot(a, b, preferred_element_type=f32)


STATE = bf16
STAGES = 4


def turned_all(narrow, wide, cosine, sine, scales):
    c, s = cosine[...], sine[...]
    parts = [turned_narrow(narrow[...].astype(f32), c, s) * scales[0]]
    for i in range(2):
        parts.append(turned_wide(wide[:, i * 128 : (i + 1) * 128].astype(f32), c, s) * scales[1])
    return [p.astype(bf16) for p in parts]


def of_head(parts, h):
    if h >= 2:
        return parts[h - 1]
    return jnp.where((lanes(parts[0].shape) // 64) == h, parts[0], jnp.zeros_like(parts[0]))


KEY_SCALES = (64**-0.5, 128**-0.5)


def state_kernel(ld, seat, kn, kw, v0, v1, cosine, sine, keep, give, state):
    length = kn.shape[0]
    keys = turned_all(kn, kw, cosine, sine, KEY_SCALES)
    t = rows((length, 128)).astype(f32)
    for h in range(4):
        g, i = h // 2, h % 2
        f, b = ld[0, g, i], ld[1, g, i]
        v = (v0 if g == 0 else v1)[:, i * 128 : (i + 1) * 128].astype(f32)
        scaled = jnp.concatenate([v * jnp.exp(f * (length - 1.0 - t)), v * jnp.exp(b * t)], 1)
        high, low = split(scaled)
        kr = keys[0] if g == 0 else keys[1 + i]
        total = tn(kr, high) + tn(kr, low)
        for d in range(2):
            part = total[:, d * 128 : (d + 1) * 128]
            if g == 0:
                state[:, d, i, :] = part[i * 64 : (i + 1) * 64]
            else:
                state[:, d, 2 + 2 * i, :] = part[:64]
                state[:, d, 3 + 2 * i, :] = part[64:]
    for d in range(2):
        for r in (6, 7):
            state[:, d, r, :] = jnp.zeros((64, 128), f32)
    keep[...] = state[pl.ds(seat[0] * 32, 32)]
    give[...] = state[pl.ds((1 - seat[0]) * 32, 32)]


def inside_kernel(ld, qn, qw, kn, kw, v0, v1, cosine, sine, turned_out, inside_out, turned, inside, sems):
    length = qn.shape[0]
    queries = turned_all(qn, qw, cosine, sine, (1.0, 1.0))
    keys = turned_all(kn, kw, cosine, sine, KEY_SCALES)
    for k in range(3):
        turned[:, k * 128 : (k + 1) * 128] = queries[k]
    turned_copy = pltpu.make_async_copy(turned, turned_out, sems.at[0])
    turned_copy.start()
    lag = (rows((length, length)) - lanes((length, length))).astype(f32)
    away = jnp.abs(lag)
    for h in range(4):
        g, i = h // 2, h % 2
        f, b = ld[0, g, i], ld[1, g, i]
        kr = keys[0] if g == 0 else keys[1 + i]
        weight = jnp.where(lag == 0, 2.0, jnp.exp(jnp.where(lag > 0, f, b) * away))
        a = (nt(of_head(queries, h), kr) * weight).astype(bf16)
        v = (v0 if g == 0 else v1)[:, i * 128 : (i + 1) * 128]
        inside[:, h * 128 : (h + 1) * 128] = nn(a, v)
    inside_copy = pltpu.make_async_copy(inside, inside_out, sems.at[1])
    inside_copy.start()
    turned_copy.wait()
    inside_copy.wait()


def finish_kernel(ld, seat, turned_in, inside_in, mine, theirs, g0, g1, out, turned, inside, enter, sems):
    copies = [
        pltpu.make_async_copy(turned_in, turned, sems.at[0]),
        pltpu.make_async_copy(inside_in, inside, sems.at[1]),
    ]
    for copy in copies:
        copy.start()
    enter[pl.ds(seat[0] * 32, 32)] = mine[...]
    enter[pl.ds((1 - seat[0]) * 32, 32)] = theirs[...]
    length = turned.shape[0]
    t = rows((length, 128)).astype(f32)
    states = []
    for h in range(4):
        g, i = h // 2, h % 2
        if g == 0:
            e = [jnp.concatenate([enter[:, d, i, :]] * 2, 0) for d in range(2)]
        else:
            e = [jnp.concatenate([enter[:, d, 2 + 2 * i, :], enter[:, d, 3 + 2 * i, :]], 0) for d in range(2)]
        states.append(split(jnp.concatenate(e, 1)))
    for copy in copies:
        copy.wait()
    queries = [turned[:, k * 128 : (k + 1) * 128] for k in range(3)]
    for h in range(4):
        g, i = h // 2, h % 2
        f, b = ld[0, g, i], ld[1, g, i]
        q = of_head(queries, h)
        high, low = states[h]
        carried = nn(q, high) + nn(q, low)
        ret = (
            inside[:, h * 128 : (h + 1) * 128]
            + carried[:, :128] * jnp.exp(f * (t + 1.0))
            + carried[:, 128:] * jnp.exp(b * (length - t))
        )
        mean = jnp.mean(ret, -1, keepdims=True)
        centred = ret - mean
        variance = jnp.mean(centred * centred, -1, keepdims=True)
        gate = (g0 if g == 0 else g1)[:, i * 128 : (i + 1) * 128].astype(f32)
        y = gate * jax.nn.sigmoid(gate) * (centred * lax.rsqrt(variance + NORM_EPSILON))
        out[:, h * 128 : (h + 1) * 128] = y.astype(bf16)


def decay_tile(ld, d, span):
    r = rows((8, 128))
    rate = jnp.full((8, 128), ld[d, 1, 1], f32)
    rate = jnp.where(r < 4, ld[d, 1, 0], rate)
    rate = jnp.where(r == 1, ld[d, 0, 1], rate)
    rate = jnp.where(r == 0, ld[d, 0, 0], rate)
    return jnp.exp(rate * span)


def pair_kernel(ld, seat, keep, got, out):
    core = seat[0]
    forward, backward = decay_tile(ld, 0, 384.0), decay_tile(ld, 1, 384.0)
    low_f = jnp.where(core == 0, keep[:, 0], got[:, 0])
    high_f = jnp.where(core == 0, got[:, 0], keep[:, 0])
    low_b = jnp.where(core == 0, keep[:, 1], got[:, 1])
    high_b = jnp.where(core == 0, got[:, 1], keep[:, 1])
    out[:, 0] = (low_f * forward[None] + high_f).astype(STATE)
    out[:, 1] = (high_b * backward[None] + low_b).astype(STATE)


def part_kernel(ld, seat, enter, keep, got, mine, theirs):
    core = seat[0]
    forward, backward = decay_tile(ld, 0, 384.0), decay_tile(ld, 1, 384.0)
    before, behind = enter[:, 0].astype(f32), enter[:, 1].astype(f32)
    low_f = jnp.where(core == 0, keep[:, 0], got[:, 0])
    high_b = jnp.where(core == 0, got[:, 1], keep[:, 1])
    second_f = before * forward[None] + low_f
    first_b = behind * backward[None] + high_b
    mine[:, 0] = jnp.where(core == 0, before, second_f)
    mine[:, 1] = jnp.where(core == 0, first_b, behind)
    theirs[:, 0] = jnp.where(core == 0, second_f, before)
    theirs[:, 1] = jnp.where(core == 0, behind, first_b)


def scan_kernel(ld, x, out):
    n = x.shape[0]
    forward, backward = decay_tile(ld, 0, 768.0), decay_tile(ld, 1, 768.0)
    acc = jnp.zeros((8, 128), f32)
    for k in range(n):
        out[k, 0] = acc.astype(STATE)
        acc = acc * forward + x[k, 0].astype(f32)
    acc = jnp.zeros((8, 128), f32)
    for k in reversed(range(n)):
        out[k, 1] = acc.astype(STATE)
        acc = acc * backward + x[k, 1].astype(f32)


def proj_kernel(place, y, stream, gain, own, *refs):
    others, (middle, normed, blocks, sems) = refs[:6], refs[6:]
    sources = [own.at[0], own.at[1], *others]
    copies = [pltpu.make_async_copy(s, blocks.at[k], sems.at[k]) for k, s in enumerate(sources)]
    for copy in copies:
        copy.start()
    tp, core = place[0], place[1]
    total = stream[...].astype(f32)
    for k, copy in enumerate(copies):
        if k < 2:
            rows_in = y[tp, :, k * 256 : (k + 1) * 256]
        else:
            piece = y[(tp + 4 - (k // 2)) % 4]
            first, _ = (core, 1 - core) if k % 2 == 0 else (1 - core, core)
            rows_in = jnp.where(first == 0, piece[:, :256], piece[:, 256:])
        copy.wait()
        part = nn(rows_in, blocks[k])
        proj = part if k == 0 else proj + part
    mid = (total + proj).astype(bf16)
    middle[...] = mid
    wide = mid.astype(f32)
    scale = lax.rsqrt(jnp.mean(wide * wide, -1, keepdims=True) + NORM_EPSILON)
    normed[...] = (wide * scale * gain[...]).astype(bf16)


SM = pl.BlockSpec(memory_space=pltpu.SMEM)
VM = pl.BlockSpec(memory_space=pltpu.VMEM)
HB = pl.BlockSpec(memory_space=pltpu.HBM)


def call(kernel, in_specs, outs, scratch=(), out_specs=None, room=40):
    return pl.pallas_call(
        kernel,
        in_specs=in_specs,
        out_specs=out_specs or jax.tree.map(lambda _: VM, outs),
        out_shape=outs,
        scratch_shapes=scratch,
        compiler_params=pltpu.CompilerParams(vmem_limit_bytes=room * 2**20),
    )


def shape(*s, dtype=f32):
    return jax.ShapeDtypeStruct(s, dtype)


def exchanged(x, axis):
    return lax.all_to_all(x, axis, 0, 0, tiled=True)


def weight_parts(width, units):
    step = width // STAGES
    spans = [pl.ds(k * step, step) for k in range(STAGES)]
    return spans, [(span, pl.ds(at, size)) for at, size in ((0, 2 * units), (2 * units, units)) for span in spans]


def mixed_into(pieces, held, outs, act, hidden, ready):
    n = pieces[0].shape[0]
    units = hidden.shape[1]
    spans, _ = weight_parts(held.shape[0], units)
    for k, span in enumerate(spans):
        x = jnp.concatenate([p[:, span] for p in pieces], 0)
        ready(k)
        part = nn(x, held[span, : 2 * units])
        act[...] = part if k == 0 else act[...] + part
    gate = act[:, :units]
    hidden[...] = (gate * jax.nn.sigmoid(gate) * act[:, units:]).astype(bf16)
    h = hidden[...]
    for k, span in enumerate(spans):
        ready(STAGES + k)
        part = nt(h, held[span, 2 * units :]).astype(bf16)
        for j, out in enumerate(outs):
            out[:, span] = part[j * n : (j + 1) * n]


def first_mixer(piece, weights, out, held, act, hidden, sems):
    _, parts = weight_parts(held.shape[0], hidden.shape[1])
    copies = [pltpu.make_async_copy(weights.at[p], held.at[p], sems.at[k]) for k, p in enumerate(parts)]
    for copy in copies:
        copy.start()
    mixed_into([piece], held, [out], act, hidden, lambda k: copies[k].wait())


def near_mixer(first, second, held, out_a, out_b, act, hidden):
    mixed_into([first, second], held, [out_a, out_b], act, hidden, lambda k: None)


def own_mixer(piece, held, out, act, hidden):
    mixed_into([piece], held, [out], act, hidden, lambda k: None)


def after(x, token):
    return lax.optimization_barrier((x, token))[0]


def in_hbm(x):
    return pltpu.with_memory_space_constraint(x, pltpu.HBM)


def in_vmem(x):
    return pltpu.with_memory_space_constraint(x, pltpu.VMEM)


def shifted(x, by):
    n = lax.axis_size("tp")
    return lax.ppermute(x, "tp", [(k, (k + by) % n) for k in range(n)])


def body(
    stream,
    query_narrow,
    key_narrow,
    query_wide,
    key_wide,
    values,
    out_gate,
    out_weight,
    norm_gain,
    mlp_gate,
    mlp_up,
    mlp_down,
    log_decay,
):
    length, width = query_narrow.shape[0], stream.shape[1]
    hidden_units = mlp_gate.shape[1]
    shards = lax.all_gather(jnp.concatenate([mlp_gate, mlp_up, mlp_down.T], 1), SP, axis=0, tiled=True)

    rates = in_hbm(log_decay)
    query_narrow, query_wide, key_narrow, key_wide = map(in_hbm, (query_narrow, query_wide, key_narrow, key_wide))
    cosine, sine = angle_tables(length, lax.axis_index(SP) * length)
    v0, v1 = values[:, 0], values[:, 1]
    g0, g1 = out_gate[:, 0], out_gate[:, 1]
    core = lax.axis_index("sp_2")
    seat = core[None].astype(jnp.int32)
    halves, states = shape(32, 2, 8, 128), shape(32, 2, 8, 128, dtype=STATE)
    keep, give = call(
        state_kernel, [SM, SM] + [VM] * 6, (halves, halves), (pltpu.VMEM((64, 2, 8, 128), f32),)
    )(rates, seat, key_narrow, key_wide, v0, v1, cosine, sine)
    got = lax.ppermute(give, "sp_2", [(0, 1), (1, 0)])
    state = call(pair_kernel, [SM, SM, VM, VM], states)(rates, seat, keep, got)
    half = lax.dynamic_index_in_dim(after(out_weight, state), core, 0, keepdims=False)
    same = []
    for s in (1, 2, 3):
        same.append(shifted(half, s))
    kept = [((length, 384), bf16), ((length, 512), f32)]
    turned, inside = call(
        inside_kernel,
        [SM] + [VM] * 8,
        tuple(pltpu.HBM(*k) for k in kept),
        tuple(pltpu.VMEM(*k) for k in kept) + (pltpu.SemaphoreType.DMA((2,)),),
        (HB, HB),
    )(rates, query_narrow, query_wide, key_narrow, key_wide, v0, v1, cosine, sine)
    arrived = exchanged(state, SP[:2])
    enter = call(scan_kernel, [SM, VM], states)(rates, arrived)
    enter = exchanged(enter, SP[:2])
    mine, theirs = call(part_kernel, [SM, SM, VM, VM, VM], (halves, halves))(rates, seat, enter, keep, got)
    theirs = lax.ppermute(theirs, "sp_2", [(0, 1), (1, 0)])
    y = call(
        finish_kernel,
        [SM, SM, HB, HB, VM, VM, VM, VM],
        shape(length, 512, dtype=bf16),
        (pltpu.VMEM((length, 384), bf16), pltpu.VMEM((length, 512), f32), pltpu.VMEM((64, 2, 8, 128), f32), pltpu.SemaphoreType.DMA((2,))),
    )(rates, seat, in_hbm(turned), in_hbm(inside), mine, theirs, g0, g1)
    other = []
    for s in (1, 2, 3):
        other.append(lax.ppermute(after(same[s - 1], y), "sp_2", [(0, 1), (1, 0)]))
    n_tp = lax.axis_size("tp")
    y = exchanged(y.reshape(n_tp, length // n_tp, 512), "tp")
    own = shape(length // n_tp, width, dtype=bf16)
    place = jnp.stack([lax.axis_index("tp"), core]).astype(jnp.int32)
    pieces = [w for pair in zip(same, other) for w in pair]
    middle, normed = call(
        proj_kernel,
        [SM, VM, VM, VM] + [HB] * 7,
        (own, own),
        (pltpu.VMEM((8, 256, width), bf16), pltpu.SemaphoreType.DMA((8,))),
    )(place, y, in_hbm(stream), in_hbm(norm_gain[None]), in_hbm(out_weight), *pieces)

    def room(pieces):
        m = pieces * own.shape[0]
        return (pltpu.VMEM((m, 2 * hidden_units), f32), pltpu.VMEM((m, hidden_units), bf16))

    around = [None] + [shifted(normed, s) for s in (1, 2, 3)]
    to_second, held = call(
        first_mixer,
        [VM, HB],
        (own, pltpu.VMEM(shards.shape, bf16)),
        room(1) + (pltpu.SemaphoreType.DMA((2 * STAGES,)),),
        room=12,
    )(around[2], in_hbm(shards))
    arrivals = [shifted(to_second, 2)]
    to_third, to_first = call(near_mixer, [VM] * 3, (own, own), room(2), room=12)(around[1], around[3], in_vmem(held))
    arrivals.append(shifted(to_third, 3))
    arrivals.append(shifted(to_first, 1))
    total = call(own_mixer, [VM] * 2, own, room(1), room=12)(after(normed, to_first), in_vmem(held))
    total = total.astype(f32)
    for arrival in arrivals:
        total = total + arrival.astype(f32)
    return (middle.astype(f32) + 0.5 * total).astype(bf16)


def solution(mesh):
    finer = Mesh(mesh.devices.reshape(8, 4, 2, mesh.shape["tp"]), ("sp_0", "sp_1", "sp_2", "tp"))
    return jax.shard_map(
        body,
        mesh=finer,
        in_specs=(
            P(SP_TP, None),
            P(SP, "tp"),
            P(SP, "tp"),
            P(SP, "tp"),
            P(SP, "tp"),
            P(SP, None, "tp"),
            P(SP, None, "tp"),
            P(None, "tp", None),
            P(),
            P(SP, "tp"),
            P(SP, "tp"),
            P("tp", SP),
            P(None, None, "tp"),
        ),
        out_specs=P(SP_TP, None),
        check_vma=False,
    )
```

```python
import jax
import jax.numpy as jnp
from jax import lax
from jax.experimental import pallas as pl
from jax.experimental.pallas import tpu as pltpu
from jax.sharding import Mesh
from jax.sharding import PartitionSpec as P


SP = ("sp_0", "sp_1", "sp_2")
SP_TP = ("sp_0", "sp_1", "sp_2", "tp")

NORM_EPSILON = 1e-06
ROPE_BASE = 10000.0
f32, bf16 = jnp.float32, jnp.bfloat16


def angle_tables(length, first):
    positions = (first + jnp.arange(length, dtype=jnp.int32)).astype(f32)
    wide = jnp.power(ROPE_BASE, -(jnp.arange(64, dtype=f32) / 64))
    narrow = jnp.power(ROPE_BASE, -(jnp.arange(32, dtype=f32) / 32))
    angles = positions[:, None] * jnp.concatenate([wide, narrow, narrow])[None]
    return jnp.cos(angles), jnp.sin(angles)


def lanes(shape):
    return lax.broadcasted_iota(jnp.int32, shape, len(shape) - 1)


def rows(shape):
    return lax.broadcasted_iota(jnp.int32, shape, 0)


def turned_wide(u, cosine, sine):
    lane = lanes(u.shape)
    c = jnp.where(lane < 64, cosine, pltpu.roll(cosine, 64, 1))
    s = jnp.where(lane < 64, -sine, pltpu.roll(sine, 64, 1))
    return u * c + pltpu.roll(u, 64, 1) * s


def turned_narrow(u, cosine, sine):
    lane = lanes(u.shape)
    c = jnp.where(lane < 64, pltpu.roll(cosine, 64, 1), cosine)
    s = jnp.where(lane < 64, pltpu.roll(sine, 64, 1), sine)
    low = (lane & 32) == 0
    other = jnp.where(low, pltpu.roll(u, 96, 1), pltpu.roll(u, 32, 1))
    return u * c + other * jnp.where(low, -s, s)


def split(x):
    high = x.astype(bf16)
    return high, (x - high.astype(f32)).astype(bf16)


def nt(a, b):
    return lax.dot_general(a, b, (((1,), (1,)), ((), ())), preferred_element_type=f32)


def tn(a, b):
    return lax.dot_general(a, b, (((0,), (0,)), ((), ())), preferred_element_type=f32)


def nn(a, b):
    return jnp.dot(a, b, preferred_element_type=f32)


STATE = bf16


def turned_all(narrow, wide, cosine, sine, scales):
    c, s = cosine[...], sine[...]
    parts = [turned_narrow(narrow[...].astype(f32), c, s) * scales[0]]
    for i in range(2):
        parts.append(turned_wide(wide[:, i * 128 : (i + 1) * 128].astype(f32), c, s) * scales[1])
    return [p.astype(bf16) for p in parts]


def of_head(parts, h):
    if h >= 2:
        return parts[h - 1]
    return jnp.where((lanes(parts[0].shape) // 64) == h, parts[0], jnp.zeros_like(parts[0]))


KEY_SCALES = (64**-0.5, 128**-0.5)


def state_kernel(ld, seat, kn, kw, v0, v1, cosine, sine, keep, give, state):
    length = kn.shape[0]
    keys = turned_all(kn, kw, cosine, sine, KEY_SCALES)
    t = rows((length, 128)).astype(f32)
    for h in range(4):
        g, i = h // 2, h % 2
        f, b = ld[0, g, i], ld[1, g, i]
        v = (v0 if g == 0 else v1)[:, i * 128 : (i + 1) * 128].astype(f32)
        scaled = jnp.concatenate([v * jnp.exp(f * (length - 1.0 - t)), v * jnp.exp(b * t)], 1)
        high, low = split(scaled)
        kr = keys[0] if g == 0 else keys[1 + i]
        total = tn(kr, high) + tn(kr, low)
        for d in range(2):
            part = total[:, d * 128 : (d + 1) * 128]
            if g == 0:
                state[:, d, i, :] = part[i * 64 : (i + 1) * 64]
            else:
                state[:, d, 2 + 2 * i, :] = part[:64]
                state[:, d, 3 + 2 * i, :] = part[64:]
    for d in range(2):
        for r in (6, 7):
            state[:, d, r, :] = jnp.zeros((64, 128), f32)
    keep[...] = state[pl.ds(seat[0] * 32, 32)]
    give[...] = state[pl.ds((1 - seat[0]) * 32, 32)]


def inside_kernel(ld, qn, qw, kn, kw, v0, v1, cosine, sine, turned_out, inside_out, turned, inside, sems):
    length = qn.shape[0]
    queries = turned_all(qn, qw, cosine, sine, (1.0, 1.0))
    keys = turned_all(kn, kw, cosine, sine, KEY_SCALES)
    for k in range(3):
        turned[:, k * 128 : (k + 1) * 128] = queries[k]
    turned_copy = pltpu.make_async_copy(turned, turned_out, sems.at[0])
    turned_copy.start()
    lag = (rows((length, length)) - lanes((length, length))).astype(f32)
    away = jnp.abs(lag)
    for h in range(4):
        g, i = h // 2, h % 2
        f, b = ld[0, g, i], ld[1, g, i]
        kr = keys[0] if g == 0 else keys[1 + i]
        weight = jnp.where(lag == 0, 2.0, jnp.exp(jnp.where(lag > 0, f, b) * away))
        a = (nt(of_head(queries, h), kr) * weight).astype(bf16)
        v = (v0 if g == 0 else v1)[:, i * 128 : (i + 1) * 128]
        inside[:, h * 128 : (h + 1) * 128] = nn(a, v)
    inside_copy = pltpu.make_async_copy(inside, inside_out, sems.at[1])
    inside_copy.start()
    turned_copy.wait()
    inside_copy.wait()


def finish_kernel(ld, seat, turned_in, inside_in, mine, theirs, g0, g1, out, turned, inside, enter, sems):
    copies = [
        pltpu.make_async_copy(turned_in, turned, sems.at[0]),
        pltpu.make_async_copy(inside_in, inside, sems.at[1]),
    ]
    for copy in copies:
        copy.start()
    enter[pl.ds(seat[0] * 32, 32)] = mine[...]
    enter[pl.ds((1 - seat[0]) * 32, 32)] = theirs[...]
    length = turned.shape[0]
    t = rows((length, 128)).astype(f32)
    states = []
    for h in range(4):
        g, i = h // 2, h % 2
        if g == 0:
            e = [jnp.concatenate([enter[:, d, i, :]] * 2, 0) for d in range(2)]
        else:
            e = [jnp.concatenate([enter[:, d, 2 + 2 * i, :], enter[:, d, 3 + 2 * i, :]], 0) for d in range(2)]
        states.append(split(jnp.concatenate(e, 1)))
    for copy in copies:
        copy.wait()
    queries = [turned[:, k * 128 : (k + 1) * 128] for k in range(3)]
    for h in range(4):
        g, i = h // 2, h % 2
        f, b = ld[0, g, i], ld[1, g, i]
        q = of_head(queries, h)
        high, low = states[h]
        carried = nn(q, high) + nn(q, low)
        ret = (
            inside[:, h * 128 : (h + 1) * 128]
            + carried[:, :128] * jnp.exp(f * (t + 1.0))
            + carried[:, 128:] * jnp.exp(b * (length - t))
        )
        mean = jnp.mean(ret, -1, keepdims=True)
        centred = ret - mean
        variance = jnp.mean(centred * centred, -1, keepdims=True)
        gate = (g0 if g == 0 else g1)[:, i * 128 : (i + 1) * 128].astype(f32)
        y = gate * jax.nn.sigmoid(gate) * (centred * lax.rsqrt(variance + NORM_EPSILON))
        out[:, h * 128 : (h + 1) * 128] = y.astype(bf16)


def decay_tile(ld, d, span):
    r = rows((8, 128))
    rate = jnp.full((8, 128), ld[d, 1, 1], f32)
    rate = jnp.where(r < 4, ld[d, 1, 0], rate)
    rate = jnp.where(r == 1, ld[d, 0, 1], rate)
    rate = jnp.where(r == 0, ld[d, 0, 0], rate)
    return jnp.exp(rate * span)


def pair_kernel(ld, seat, keep, got, out):
    core = seat[0]
    forward, backward = decay_tile(ld, 0, 384.0), decay_tile(ld, 1, 384.0)
    low_f = jnp.where(core == 0, keep[:, 0], got[:, 0])
    high_f = jnp.where(core == 0, got[:, 0], keep[:, 0])
    low_b = jnp.where(core == 0, keep[:, 1], got[:, 1])
    high_b = jnp.where(core == 0, got[:, 1], keep[:, 1])
    out[:, 0] = (low_f * forward[None] + high_f).astype(STATE)
    out[:, 1] = (high_b * backward[None] + low_b).astype(STATE)


def part_kernel(ld, seat, enter, keep, got, mine, theirs):
    core = seat[0]
    forward, backward = decay_tile(ld, 0, 384.0), decay_tile(ld, 1, 384.0)
    before, behind = enter[:, 0].astype(f32), enter[:, 1].astype(f32)
    low_f = jnp.where(core == 0, keep[:, 0], got[:, 0])
    high_b = jnp.where(core == 0, got[:, 1], keep[:, 1])
    second_f = before * forward[None] + low_f
    first_b = behind * backward[None] + high_b
    mine[:, 0] = jnp.where(core == 0, before, second_f)
    mine[:, 1] = jnp.where(core == 0, first_b, behind)
    theirs[:, 0] = jnp.where(core == 0, second_f, before)
    theirs[:, 1] = jnp.where(core == 0, behind, first_b)


def scan_kernel(ld, x, out):
    n = x.shape[0]
    forward, backward = decay_tile(ld, 0, 768.0), decay_tile(ld, 1, 768.0)
    acc = jnp.zeros((8, 128), f32)
    for k in range(n):
        out[k, 0] = acc.astype(STATE)
        acc = acc * forward + x[k, 0].astype(f32)
    acc = jnp.zeros((8, 128), f32)
    for k in reversed(range(n)):
        out[k, 1] = acc.astype(STATE)
        acc = acc * backward + x[k, 1].astype(f32)


def proj_kernel(place, y, stream, gain, own, *refs):
    others, (middle, normed, blocks, sems) = refs[:6], refs[6:]
    sources = [own.at[0], own.at[1], *others]
    copies = [pltpu.make_async_copy(s, blocks.at[k], sems.at[k]) for k, s in enumerate(sources)]
    for copy in copies:
        copy.start()
    tp, core = place[0], place[1]
    total = stream[...].astype(f32)
    for k, copy in enumerate(copies):
        if k < 2:
            rows_in = y[tp, :, k * 256 : (k + 1) * 256]
        else:
            piece = y[(tp + 4 - (k // 2)) % 4]
            first, _ = (core, 1 - core) if k % 2 == 0 else (1 - core, core)
            rows_in = jnp.where(first == 0, piece[:, :256], piece[:, 256:])
        copy.wait()
        part = nn(rows_in, blocks[k])
        proj = part if k == 0 else proj + part
    mid = (total + proj).astype(bf16)
    middle[...] = mid
    wide = mid.astype(f32)
    scale = lax.rsqrt(jnp.mean(wide * wide, -1, keepdims=True) + NORM_EPSILON)
    normed[...] = (wide * scale * gain[...]).astype(bf16)


SM = pl.BlockSpec(memory_space=pltpu.SMEM)
VM = pl.BlockSpec(memory_space=pltpu.VMEM)
HB = pl.BlockSpec(memory_space=pltpu.HBM)


def call(kernel, in_specs, outs, scratch=(), out_specs=None, room=40):
    return pl.pallas_call(
        kernel,
        in_specs=in_specs,
        out_specs=out_specs or jax.tree.map(lambda _: VM, outs),
        out_shape=outs,
        scratch_shapes=scratch,
        compiler_params=pltpu.CompilerParams(vmem_limit_bytes=room * 2**20),
    )


def shape(*s, dtype=f32):
    return jax.ShapeDtypeStruct(s, dtype)


def exchanged(x, axis):
    return lax.all_to_all(x, axis, 0, 0, tiled=True)


RISING = (512, 512, 512, 256, 256)
FALLING = (512, 512, 512, 512)


def row_spans(sizes):
    return [pl.ds(sum(sizes[:k]), size) for k, size in enumerate(sizes)]


def weight_parts(units):
    rising = [(span, pl.ds(0, 2 * units)) for span in row_spans(RISING)]
    return rising + [(span, pl.ds(2 * units, units)) for span in row_spans(FALLING)]


def mixed_into(pieces, held, outs, act, hidden, ready):
    n = pieces[0].shape[0]
    units = hidden.shape[1]
    for k, span in enumerate(row_spans(RISING)):
        x = jnp.concatenate([p[:, span] for p in pieces], 0)
        ready(k)
        part = nn(x, held[span, : 2 * units])
        act[...] = part if k == 0 else act[...] + part
    gate = act[:, :units]
    hidden[...] = (gate * jax.nn.sigmoid(gate) * act[:, units:]).astype(bf16)
    h = hidden[...]
    for k, span in enumerate(row_spans(FALLING)):
        ready(len(RISING) + k)
        part = nt(h, held[span, 2 * units :]).astype(bf16)
        for j, out in enumerate(outs):
            out[:, span] = part[j * n : (j + 1) * n]


def first_mixer(piece, weights, out, held, act, hidden, sems):
    parts = weight_parts(hidden.shape[1])
    copies = [pltpu.make_async_copy(weights.at[p], held.at[p], sems.at[k]) for k, p in enumerate(parts)]
    for copy in copies:
        copy.start()
    mixed_into([piece], held, [out], act, hidden, lambda k: copies[k].wait())


def near_mixer(first, second, held, out_a, out_b, act, hidden):
    mixed_into([first, second], held, [out_a, out_b], act, hidden, lambda k: None)


def own_mixer(piece, held, out, act, hidden):
    mixed_into([piece], held, [out], act, hidden, lambda k: None)


def after(x, token):
    return lax.optimization_barrier((x, token))[0]


def in_hbm(x):
    return pltpu.with_memory_space_constraint(x, pltpu.HBM)


def in_vmem(x):
    return pltpu.with_memory_space_constraint(x, pltpu.VMEM)


def shifted(x, by):
    n = lax.axis_size("tp")
    return lax.ppermute(x, "tp", [(k, (k + by) % n) for k in range(n)])


def body(
    stream,
    query_narrow,
    key_narrow,
    query_wide,
    key_wide,
    values,
    out_gate,
    out_weight,
    norm_gain,
    mlp_gate,
    mlp_up,
    mlp_down,
    log_decay,
):
    length, width = query_narrow.shape[0], stream.shape[1]
    hidden_units = mlp_gate.shape[1]
    shards = lax.all_gather(jnp.concatenate([mlp_gate, mlp_up, mlp_down.T], 1), SP, axis=0, tiled=True)

    rates = in_hbm(log_decay)
    query_narrow, query_wide, key_narrow, key_wide = map(in_hbm, (query_narrow, query_wide, key_narrow, key_wide))
    cosine, sine = angle_tables(length, lax.axis_index(SP) * length)
    v0, v1 = values[:, 0], values[:, 1]
    g0, g1 = out_gate[:, 0], out_gate[:, 1]
    core = lax.axis_index("sp_2")
    seat = core[None].astype(jnp.int32)
    halves, states = shape(32, 2, 8, 128), shape(32, 2, 8, 128, dtype=STATE)
    keep, give = call(
        state_kernel, [SM, SM] + [VM] * 6, (halves, halves), (pltpu.VMEM((64, 2, 8, 128), f32),)
    )(rates, seat, key_narrow, key_wide, v0, v1, cosine, sine)
    got = lax.ppermute(give, "sp_2", [(0, 1), (1, 0)])
    state = call(pair_kernel, [SM, SM, VM, VM], states)(rates, seat, keep, got)
    half = lax.dynamic_index_in_dim(after(out_weight, state), core, 0, keepdims=False)
    same = []
    for s in (1, 2, 3):
        same.append(shifted(half, s))
    kept = [((length, 384), bf16), ((length, 512), f32)]
    turned, inside = call(
        inside_kernel,
        [SM] + [VM] * 8,
        tuple(pltpu.HBM(*k) for k in kept),
        tuple(pltpu.VMEM(*k) for k in kept) + (pltpu.SemaphoreType.DMA((2,)),),
        (HB, HB),
    )(rates, query_narrow, query_wide, key_narrow, key_wide, v0, v1, cosine, sine)
    arrived = exchanged(state, SP[:2])
    enter = call(scan_kernel, [SM, VM], states)(rates, arrived)
    enter = exchanged(enter, SP[:2])
    mine, theirs = call(part_kernel, [SM, SM, VM, VM, VM], (halves, halves))(rates, seat, enter, keep, got)
    theirs = lax.ppermute(theirs, "sp_2", [(0, 1), (1, 0)])
    y = call(
        finish_kernel,
        [SM, SM, HB, HB, VM, VM, VM, VM],
        shape(length, 512, dtype=bf16),
        (pltpu.VMEM((length, 384), bf16), pltpu.VMEM((length, 512), f32), pltpu.VMEM((64, 2, 8, 128), f32), pltpu.SemaphoreType.DMA((2,))),
    )(rates, seat, in_hbm(turned), in_hbm(inside), mine, theirs, g0, g1)
    other = []
    for s in (1, 2, 3):
        other.append(lax.ppermute(after(same[s - 1], y), "sp_2", [(0, 1), (1, 0)]))
    n_tp = lax.axis_size("tp")
    y = exchanged(y.reshape(n_tp, length // n_tp, 512), "tp")
    own = shape(length // n_tp, width, dtype=bf16)
    place = jnp.stack([lax.axis_index("tp"), core]).astype(jnp.int32)
    pieces = [w for pair in zip(same, other) for w in pair]
    middle, normed = call(
        proj_kernel,
        [SM, VM, VM, VM] + [HB] * 7,
        (own, own),
        (pltpu.VMEM((8, 256, width), bf16), pltpu.SemaphoreType.DMA((8,))),
    )(place, y, in_hbm(stream), in_hbm(norm_gain[None]), in_hbm(out_weight), *pieces)

    def room(pieces):
        m = pieces * own.shape[0]
        return (pltpu.VMEM((m, 2 * hidden_units), f32), pltpu.VMEM((m, hidden_units), bf16))

    around = [None] + [shifted(normed, s) for s in (1, 2, 3)]
    to_second, held = call(
        first_mixer,
        [VM, HB],
        (own, pltpu.VMEM(shards.shape, bf16)),
        room(1) + (pltpu.SemaphoreType.DMA((len(RISING) + len(FALLING),)),),
        room=12,
    )(around[2], in_hbm(shards))
    arrivals = [shifted(to_second, 2)]
    to_third, to_first = call(near_mixer, [VM] * 3, (own, own), room(2), room=12)(around[1], around[3], in_vmem(held))
    arrivals.append(shifted(to_third, 3))
    arrivals.append(shifted(to_first, 1))
    total = call(own_mixer, [VM] * 2, own, room(1), room=12)(after(normed, to_first), in_vmem(held))
    total = total.astype(f32)
    for arrival in arrivals:
        total = total + arrival.astype(f32)
    return (middle.astype(f32) + 0.5 * total).astype(bf16)


def solution(mesh):
    finer = Mesh(mesh.devices.reshape(8, 4, 2, mesh.shape["tp"]), ("sp_0", "sp_1", "sp_2", "tp"))
    return jax.shard_map(
        body,
        mesh=finer,
        in_specs=(
            P(SP_TP, None),
            P(SP, "tp"),
            P(SP, "tp"),
            P(SP, "tp"),
            P(SP, "tp"),
            P(SP, None, "tp"),
            P(SP, None, "tp"),
            P(None, "tp", None),
            P(),
            P(SP, "tp"),
            P(SP, "tp"),
            P("tp", SP),
            P(None, None, "tp"),
        ),
        out_specs=P(SP_TP, None),
        check_vma=False,
    )
```
